256 devices in a mesh: grp: 2 (over y), sp: 32 (over z, core), tp: 4 (over x).
Axes of the slice: x: 4, y: 2, z: 16, core: 2. Of those that a mesh axis runs over, the one named last changes fastest.
The devices are a block of a 4x16x16 slice.
Arguments:
- stream_in: bfloat16 [32768, 2048], P(('grp', 'sp')), parts along dimension 0, may hold values from -6 to 6
- query_wide: bfloat16 [32768, 1024], P(('grp', 'sp'), 'tp'), parts along dimension 0, may hold values from -6 to 6
- key_wide: bfloat16 [32768, 1024], P(('grp', 'sp'), 'tp'), parts along dimension 0, may hold values from -6 to 6
- value_wide: bfloat16 [32768, 2048], P(('grp', 'sp'), 'tp'), parts along dimension 0, may hold values from -6 to 6
- query_narrow: bfloat16 [32768, 512], P(('grp', 'sp'), 'tp'), parts along dimension 0, may hold values from -6 to 6
- key_narrow: bfloat16 [32768, 512], P(('grp', 'sp'), 'tp'), parts along dimension 0, may hold values from -6 to 6
- value_narrow: bfloat16 [32768, 1024], P(('grp', 'sp'), 'tp'), parts along dimension 0, may hold values from -6 to 6
- decay_wide: float32 [4, 32768], P('tp', ('grp', 'sp')), parts along dimension 1, may hold values from -1 to 0
- decay_narrow: float32 [4, 32768], P('tp', ('grp', 'sp')), parts along dimension 1, may hold values from -1 to 0
- gain_wide: float32 [2048], P('tp'), may hold values from 0.1 to 1.9
- gain_narrow: float32 [1024], P('tp'), may hold values from 0.1 to 1.9
- out_wide: bfloat16 [2048, 2048], P('tp'), may hold values from -0.109375 to 0.109375
- out_narrow: bfloat16 [1024, 2048], P('tp'), may hold values from -0.109375 to 0.109375
- mlp_gain: float32 [2048], replicated, may hold values from 0.1 to 1.9
- up_weight: bfloat16 [2048, 8192], P('sp', 'tp'), may hold values from -0.125 to 0.125
- down_weight: bfloat16 [8192, 2048], P('tp', 'sp'), may hold values from -0.0625 to 0.0625
Outputs:
- stream_out: bfloat16 [32768, 2048], P(('grp', 'sp', 'tp')), parts along dimension 0
The draws below stay inside these ranges and needn't reach their ends.
There are 2 independent parts, one for each index of `grp`. The reference program is written for one: setup_inputs(seed, part) draws one part's arguments, and reference() takes and returns one part's arrays. A program takes and returns all parts, laid end to end along the dimension named above; an argument that names none is the same for every part. Nothing has to cross between parts.
All inputs are finite; a program needn't handle non-finite values.
Results may differ from the reference program's by a relative error of at most 0.019.
Values may be sent and summed in bfloat16 or wider, within the bound.
No kernel may reach another device: no remote copies, remote signals or barrier semaphores. Data moves between devices by JAX's collectives and lax.ppermute only.
A program may use at most 128 MiB of HBM per device.

```python
import math
import jax
import jax.numpy as jnp
from jax import lax

D = 2048
FF = 8192
HW = 4
HN = 4
DKW = 256
DVW = 512
DKN = 128
DVN = 256
TOK_DEV = 512
SEQUENCE_LENGTH = 16384
N_TP = 4


def decay_table(key, total_heads):
    shard_total = jax.random.split(key, 6)
    slow = jax.random.permutation(shard_total[0], total_heads) < total_heads // 2
    fast_rate = jnp.exp(jax.random.uniform(shard_total[1], (total_heads, 1), jnp.float32, math.log(1.0 / 50.0), math.log(1.0 / 30.0)))
    slow_rate = 0.4 / SEQUENCE_LENGTH
    block_factor = jnp.exp(jax.random.uniform(shard_total[2], (1, SEQUENCE_LENGTH // TOK_DEV), jnp.float32, math.log(0.5), math.log(2.0)))
    block_factor = jnp.repeat(block_factor, TOK_DEV, axis=1)
    roughness = jax.random.uniform(shard_total[3], (total_heads, SEQUENCE_LENGTH), jnp.float32, 0.5, 1.5)
    decay_rate = jnp.where(slow[:, None], slow_rate * block_factor, fast_rate * jnp.ones((1, SEQUENCE_LENGTH), jnp.float32))
    decay_rate = decay_rate * roughness
    segment_offset = jax.random.randint(shard_total[4], (total_heads, 2), 0, SEQUENCE_LENGTH)
    segment_length = jax.random.uniform(shard_total[5], (total_heads, 2), jnp.float32, math.log(0.5), math.log(0.8))
    token_position = jnp.arange(SEQUENCE_LENGTH, dtype=jnp.int32)
    segment_count = jnp.sum(jnp.where(token_position[None, None, :] == segment_offset[:, :, None], segment_length[:, :, None], 0.0), axis=1)
    return (segment_count - decay_rate).astype(jnp.float32)


def draw_decay_wide(key, part):
    return decay_table(jax.random.fold_in(key, 11), HW)


def draw_decay_narrow(key, part):
    return decay_table(jax.random.fold_in(key, 23), HN)


def block_scale(key, dims, shards, low, top_value):
    gain = 1.0
    for position, shards_of in shards:
        heights = jax.random.uniform(jax.random.fold_in(jax.random.fold_in(key, 6), position), (shards_of,), jnp.float32, low / len(shards), top_value / len(shards))
        gain = gain * jnp.repeat(jnp.exp(heights), dims[position] // shards_of).reshape((-1,) + (1,) * (len(dims) - 1 - position))
    return gain


def centred(key, dims, width, most, shards=(), kind=jnp.bfloat16):
    drawn = jax.random.normal(key, dims, jnp.float32) * width
    if len(shards) > 0:
        drawn = block_scale(key, dims, shards, -0.22, 0.18) * drawn
    return jnp.clip(drawn, min=-most, max=most).astype(kind)


def setup_inputs(seed: int = 0, part: int = 0) -> dict:
    splits = jax.random.split(jax.random.key(seed), 17)
    part_splits = jax.random.split(jax.random.fold_in(splits[16], part), 17)
    stream_in = centred(part_splits[0], (SEQUENCE_LENGTH, D), 1.0, 6.0, ((0, 32),))
    query_wide = centred(part_splits[1], (SEQUENCE_LENGTH, HW * DKW), 1.0, 6.0, ((0, 32), (1, 4)))
    key_wide = centred(part_splits[2], (SEQUENCE_LENGTH, HW * DKW), 1.0, 6.0, ((0, 32), (1, 4)))
    value_wide = centred(part_splits[3], (SEQUENCE_LENGTH, HW * DVW), 1.0, 6.0, ((0, 32), (1, 4)))
    query_narrow = centred(part_splits[4], (SEQUENCE_LENGTH, HN * DKN), 1.0, 6.0, ((0, 32), (1, 4)))
    key_narrow = centred(part_splits[5], (SEQUENCE_LENGTH, HN * DKN), 1.0, 6.0, ((0, 32), (1, 4)))
    value_narrow = centred(part_splits[6], (SEQUENCE_LENGTH, HN * DVN), 1.0, 6.0, ((0, 32), (1, 4)))
    decay_wide = draw_decay_wide(jax.random.fold_in(jax.random.fold_in(splits[16], part), 71), part)
    decay_narrow = draw_decay_narrow(jax.random.fold_in(jax.random.fold_in(splits[16], part), 71), part)
    gain_wide = jnp.clip(1.0 + 0.18 * jax.random.normal(splits[9], (HW * DVW,), jnp.float32), 0.1, 1.9)
    gain_narrow = jnp.clip(1.0 + 0.18 * jax.random.normal(splits[10], (HN * DVN,), jnp.float32), 0.1, 1.9)
    out_wide = centred(splits[11], (HW * DVW, D), (HW * DVW + HN * DVN) ** -0.5, 0.109375, ((0, 4),))
    out_narrow = centred(splits[12], (HN * DVN, D), (HW * DVW + HN * DVN) ** -0.5, 0.109375, ((0, 4),))
    mlp_gain = jnp.clip(1.0 + 0.18 * jax.random.normal(splits[13], (D,), jnp.float32), 0.1, 1.9)
    up_weight = centred(splits[14], (D, FF), D ** -0.5, 0.125, ((0, 32), (1, 4)))
    down_weight = centred(splits[15], (FF, D), FF ** -0.5, 0.0625, ((0, 4), (1, 32)))
    return dict(stream_in=stream_in, query_wide=query_wide, key_wide=key_wide, value_wide=value_wide, query_narrow=query_narrow, key_narrow=key_narrow, value_narrow=value_narrow, decay_wide=decay_wide, decay_narrow=decay_narrow, gain_wide=gain_wide, gain_narrow=gain_narrow, out_wide=out_wide, out_narrow=out_narrow, mlp_gain=mlp_gain, up_weight=up_weight, down_weight=down_weight)


EPS = 1e-06

def retain_group(queries, key_rows, value_rows, log_decay):
    total_heads = log_decay.shape[0]
    length = queries.shape[0]
    key_width = queries.shape[1] // total_heads
    value_width = value_rows.shape[1] // total_heads
    block_count = length // TOK_DEV
    query_blocks = queries.reshape(block_count, TOK_DEV, total_heads, key_width)
    key_blocks = key_rows.reshape(block_count, TOK_DEV, total_heads, key_width)
    value_blocks = value_rows.reshape(block_count, TOK_DEV, total_heads, value_width)
    decay_blocks = log_decay.reshape(total_heads, block_count, TOK_DEV).transpose(1, 0, 2)
    row_index = lax.broadcasted_iota(jnp.int32, (TOK_DEV, TOK_DEV), 0)
    col_index = lax.broadcasted_iota(jnp.int32, (TOK_DEV, TOK_DEV), 1)
    causal = (row_index >= col_index)[None]

    def advance(state, inputs):
        query_here, key_here, value_here, decay_here = inputs
        cumulative = jnp.cumsum(decay_here, axis=1)
        log_gap = cumulative[:, :, None] - cumulative[:, None, :]
        fading = jnp.where(causal, jnp.exp(jnp.where(causal, log_gap, 0.0)), 0.0)
        scores = jnp.einsum('ihd,jhd->hij', query_here.astype(jnp.float32), key_here.astype(jnp.float32))
        weights_low = lax.optimization_barrier((scores * key_width ** (-0.5) * fading).astype(jnp.bfloat16))
        within = jnp.einsum('hij,jhe->ihe', weights_low.astype(jnp.float32), value_here.astype(jnp.float32))
        carried = jnp.einsum('ihd,hde->ihe', query_here.astype(jnp.float32), state, precision=lax.Precision.HIGHEST) * jnp.exp(cumulative).T[:, :, None]
        to_end = jnp.exp(cumulative[:, -1:] - cumulative)
        keyed = lax.optimization_barrier((key_here.astype(jnp.float32) * key_width ** (-0.5) * to_end.T[:, :, None]).astype(jnp.bfloat16))
        local_state = jnp.einsum('jhd,jhe->hde', keyed.astype(jnp.float32), value_here.astype(jnp.float32))
        updated = jnp.exp(cumulative[:, -1])[:, None, None] * state + local_state
        return (updated, within + carried)
    start_state = jnp.zeros((total_heads, key_width, value_width), jnp.float32)
    _, retained = lax.scan(advance, start_state, (query_blocks, key_blocks, value_blocks, decay_blocks))
    return retained.reshape(length, total_heads, value_width)

def head_norm(retained, gain_values):
    centered = retained - lax.optimization_barrier(jnp.mean(retained, axis=-1, keepdims=True))
    scaled = centered * lax.rsqrt(lax.optimization_barrier(jnp.mean(centered * centered, axis=-1, keepdims=True)) + EPS)
    return (scaled.reshape(retained.shape[0], -1) * gain_values).astype(jnp.bfloat16)

def normalize(rows, gain_values):
    values = rows.astype(jnp.float32)
    scaled = values * lax.rsqrt(lax.optimization_barrier(jnp.mean(values * values, axis=-1, keepdims=True)) + EPS)
    return (scaled * gain_values).astype(jnp.bfloat16)

def reference(stream_in, query_wide, key_wide, value_wide, query_narrow, key_narrow, value_narrow, decay_wide, decay_narrow, gain_wide, gain_narrow, out_wide, out_narrow, mlp_gain, up_weight, down_weight):
    normed_wide = head_norm(retain_group(query_wide, key_wide, value_wide, decay_wide), gain_wide)
    normed_narrow = head_norm(retain_group(query_narrow, key_narrow, value_narrow, decay_narrow), gain_narrow)
    wide_cols = normed_wide.shape[1] // N_TP
    narrow_cols = normed_narrow.shape[1] // N_TP
    mix = jnp.zeros(stream_in.shape, jnp.float32)
    for member in range(N_TP):
        partial_sum = jnp.dot(normed_wide[:, member * wide_cols:(member + 1) * wide_cols], out_wide[member * wide_cols:(member + 1) * wide_cols], preferred_element_type=jnp.float32)
        partial_sum = partial_sum + jnp.dot(normed_narrow[:, member * narrow_cols:(member + 1) * narrow_cols], out_narrow[member * narrow_cols:(member + 1) * narrow_cols], preferred_element_type=jnp.float32)
        mix = mix + partial_sum.astype(jnp.bfloat16).astype(jnp.float32)
    middle = (stream_in.astype(jnp.float32) + mix).astype(jnp.bfloat16)
    normed_rows = normalize(middle, mlp_gain)
    hidden = jax.nn.relu(jnp.dot(normed_rows, up_weight, preferred_element_type=jnp.float32))
    hidden = (hidden * hidden).astype(jnp.bfloat16)
    unit_cols = hidden.shape[1] // N_TP
    channel = jnp.zeros(stream_in.shape, jnp.float32)
    for member in range(N_TP):
        partial_sum = jnp.dot(hidden[:, member * unit_cols:(member + 1) * unit_cols], down_weight[member * unit_cols:(member + 1) * unit_cols], preferred_element_type=jnp.float32)
        channel = channel + partial_sum.astype(jnp.bfloat16).astype(jnp.float32)
    return (middle.astype(jnp.float32) + channel).astype(jnp.bfloat16)
```

```python
import jax
import jax.numpy as jnp
from jax import lax
from jax.experimental import pallas as pl
from jax.experimental.pallas import tpu as pltpu
from jax.sharding import Mesh
from jax.sharding import PartitionSpec as P

EPS = 1e-06
SP = ("za", "zb", "core")
GRP_SP = ("grp", "za", "zb", "core")
GRP_SP_TP = ("grp", "za", "zb", "core", "tp")
F32 = jnp.float32
BF16 = jnp.bfloat16
LANES = 128


def vmem():
    return pl.BlockSpec(memory_space=pltpu.VMEM)


def smem():
    return pl.BlockSpec(memory_space=pltpu.SMEM)


def call(body, outs, *args, scratch=(), flops=0, moved=0):
    specs = [smem() if a.dtype == jnp.int32 else vmem() for a in args]
    many = isinstance(outs, (list, tuple))
    return pl.pallas_call(
        body,
        out_shape=outs,
        in_specs=specs,
        out_specs=[vmem() for _ in outs] if many else vmem(),
        scratch_shapes=list(scratch),
        compiler_params=pltpu.CompilerParams(vmem_limit_bytes=48 * 2**20),
        cost_estimate=pl.CostEstimate(flops=flops, bytes_accessed=moved, transcendentals=0),
        name=body.__name__,
    )(*args)


def shaped(shape, dtype):
    return jax.ShapeDtypeStruct(shape, dtype)


def mm(a, b, dims=((1,), (0,))):
    return lax.dot_general(a, b, (dims, ((), ())), preferred_element_type=F32)


def three(x):
    high = x.astype(BF16).astype(F32)
    mid = (x - high).astype(BF16).astype(F32)
    low = (x - high - mid).astype(BF16).astype(F32)
    return high, mid, low


def pick(index, values):
    out = jnp.zeros_like(index, dtype=F32)
    for n, value in enumerate(values):
        out = jnp.where(index == n, value, out)
    return out


def decay_rows(dw, dn):
    row = lax.broadcasted_iota(jnp.int32, (8, dw.shape[1]), 0)
    return pick(row, three(dw) + three(dn)).astype(BF16)


def columns(table):
    wide = table[:, 0:1] + table[:, 1:2] + table[:, 2:3]
    thin = table[:, 3:4] + table[:, 4:5] + table[:, 5:6]
    return wide, thin


def log_lanes(wide, thin, rows):
    lane = lax.broadcasted_iota(jnp.int32, (rows, LANES), 1)
    return pick(lane, three(wide) + three(thin))


def positions(length):
    row = lax.broadcasted_iota(jnp.int32, (length, length), 0)
    col = lax.broadcasted_iota(jnp.int32, (length, length), 1)
    return row, col


def own_state(kw, vw, dw, kn, vn, dn, out):
    length = kw.shape[0]
    row, col = positions(length)
    later = (col > row).astype(F32).astype(BF16)
    table = decay_rows(dw[...], dn[...])
    end_wide, end_thin = columns(mm(later, table, ((1,), (1,))))
    total_wide = jnp.sum(dw[...], axis=1, keepdims=True)
    total_thin = jnp.sum(dn[...], axis=1, keepdims=True)

    def state(k, v, end):
        keyed = k[...].astype(F32) * k.shape[1] ** (-0.5) * jnp.exp(end)
        return mm(keyed.astype(BF16), v[...], ((0,), (0,))).astype(BF16)

    wide = state(kw, vw, end_wide)
    thin = state(kn, vn, end_thin)
    half_wide, half_thin = wide.shape[0] // 2, thin.shape[0] // 2
    at = wide.shape[1]
    logs = log_lanes(total_wide, total_thin, half_wide).astype(BF16)
    for h in range(2):
        out[h, :, :at] = wide[h * half_wide : (h + 1) * half_wide]
        part = thin[h * half_thin : (h + 1) * half_thin]
        out[h, :half_thin, at : at + LANES] = part[:, :LANES]
        out[h, half_thin:, at : at + LANES] = part[:, LANES:]
        out[h, :, at + LANES :] = logs


def inside(qw, kw, vw, dw, qn, kn, vn, dn, out):
    length = kw.shape[0]
    row, col = positions(length)
    causal = row >= col
    upto = causal.astype(F32).astype(BF16)
    table = decay_rows(dw[...], dn[...])
    col_wide, col_thin = columns(mm(upto, table, ((1,), (1,))))
    rows = mm(table, upto, ((1,), (1,)))
    row_wide = rows[0:1] + rows[1:2] + rows[2:3]
    row_thin = rows[3:4] + rows[4:5] + rows[5:6]

    def within(q, k, v, by_col, by_row):
        gap = jnp.where(causal, by_col - by_row, 0.0)
        fading = jnp.where(causal, jnp.exp(gap), 0.0)
        weights = mm(q[...], k[...], ((1,), (1,))) * k.shape[1] ** (-0.5) * fading
        return mm(weights.astype(BF16), v[...])

    at = vw.shape[1]
    out[:, :at] = within(qw, kw, vw, col_wide, row_wide)
    out[:, at:] = within(qn, kn, vn, col_thin, row_thin)


def unpack(x):
    x = x.astype(F32)
    cut = x.shape[-1] - LANES
    wide, thin = columns(x[:, cut:])
    return x[:, : cut - LANES], x[:, cut - LANES : cut], wide, thin


def after(earlier, latter):
    return (
        jnp.exp(latter[2]) * earlier[0] + latter[0],
        jnp.exp(latter[3]) * earlier[1] + latter[1],
        earlier[2] + latter[2],
        earlier[3] + latter[3],
    )


def put(ref, at, state, logs=True):
    rows, wide, thin = state[0].shape[0], state[0].shape[1], state[1].shape[1]
    ref[at, :, :wide] = state[0].astype(BF16)
    ref[at, :, wide : wide + thin] = state[1].astype(BF16)
    if logs:
        ref[at, :, wide + thin :] = log_lanes(state[2], state[3], rows).astype(BF16)


def of_chip(place, own, sibling, out):
    core, spot = place[0], place[1]
    first_core = core == 0
    pieces, rows = out.shape[0], out.shape[1]
    for d in range(pieces):
        start = pl.multiple_of(lax.rem(spot + d, pieces) * rows, rows)
        mine = own[core, pl.ds(start, rows), :]
        other = sibling[core, pl.ds(start, rows), :]
        first = jnp.where(first_core, mine, other)
        second = jnp.where(first_core, other, mine)
        put(out, d, after(unpack(first), unpack(second)))


def in_order(place, parts, ordered):
    pieces = len(parts)
    for d, part in enumerate(parts):
        ordered[lax.rem(place[1] - d + pieces, pieces)] = part[...]


def of_group(place, a, b, c, d, out, ordered):
    in_order(place, (a, b, c, d), ordered)
    total = unpack(ordered[0])
    for n in range(1, 4):
        total = after(total, unpack(ordered[n]))
    put(out, 0, total)


def before_each(place, a, b, c, d, near, mid, far, out, ordered, found):
    in_order(place, (a, b, c, d), ordered)
    state = after(after(unpack(far[0]), unpack(mid[0])), unpack(near[0]))
    for n in range(4):
        put(found, n, state, logs=False)
        state = after(state, unpack(ordered[n]))
    for n in range(4):
        out[n] = found[lax.rem(place[1] + n, 4)]


def gathered_half(place, a, b, c, d, out):
    parts = (a, b, c, d)
    rows = a.shape[0]
    for n, part in enumerate(parts):
        start = pl.multiple_of(lax.rem(place[1] - n + 4, 4) * rows, rows)
        out[pl.ds(start, rows), :] = part[...]


def heads_out(
    place, own_half, other_half, sibling, qw, qn, dw, dn, within, gw, gn, ow, on, out,
    came_wide, came_thin,
):
    first_core = place[0] == 0
    length = qw.shape[0]
    wide_width, thin_width = gw.shape[1], gn.shape[1]
    half_thin = came_thin.shape[0] // 2
    rows = own_half.shape[0]
    for h in range(2):
        mine = own_half[...] if h == 0 else other_half[...]
        other = other_half[...] if h == 0 else own_half[...]
        before = jnp.where(first_core, mine, other).astype(F32)
        s_wide, s_thin, l_wide, l_thin = unpack(sibling[h])
        b_wide, b_thin = before[:, :wide_width], before[:, wide_width:]
        wide = jnp.where(first_core, b_wide, jnp.exp(l_wide) * b_wide + s_wide)
        thin = jnp.where(first_core, b_thin, jnp.exp(l_thin) * b_thin + s_thin)
        came_wide[h * rows : (h + 1) * rows, :] = wide.astype(BF16)
        low = thin.astype(BF16)
        came_thin[h * half_thin : (h + 1) * half_thin, :LANES] = low[:half_thin]
        came_thin[h * half_thin : (h + 1) * half_thin, LANES:] = low[half_thin:]
    row, col = positions(length)
    upto = (row >= col).astype(F32).astype(BF16)
    cum_wide, cum_thin = columns(mm(upto, decay_rows(dw[...], dn[...]), ((1,), (1,))))

    def normed(q, came, cum, inner, gain):
        kept = inner + mm(q[...], came[...]) * jnp.exp(cum)
        centered = kept - jnp.mean(kept, axis=-1, keepdims=True)
        power = jnp.mean(centered * centered, axis=-1, keepdims=True)
        return (centered * lax.rsqrt(power + EPS) * gain[...]).astype(BF16)

    wide = normed(qw, came_wide, cum_wide, within[:, :wide_width], gw)
    thin = normed(qn, came_thin, cum_thin, within[:, wide_width:], gn)
    step = 512
    for n in range(ow.shape[1] // step):
        cols = slice(n * step, (n + 1) * step)
        out[:, cols] = (mm(wide, ow[:, cols]) + mm(thin, on[:, cols])).astype(BF16)


def rows_mid(parts, stream, gain, middle, normed):
    total = parts[0].astype(F32)
    for n in range(1, parts.shape[0]):
        total = total + parts[n].astype(F32)
    mid = (stream[...].astype(F32) + total).astype(BF16)
    middle[...] = mid
    values = mid.astype(F32)
    power = jnp.mean(values * values, axis=-1, keepdims=True)
    normed[...] = (values * lax.rsqrt(power + EPS) * gain[...]).astype(BF16)


def shift(x, axis, by, size, wrap=True):
    pairs = [(i, (i + by) % size) for i in range(size) if wrap or 0 <= i + by < size]
    return lax.ppermute(x, axis, pairs)


def swap(x):
    return lax.ppermute(x, "core", [(0, 1), (1, 0)])


def among(parts):
    return [parts[0]] + [shift(parts[d], "zb", d, 4) for d in range(1, 4)]


def on_device(
    stream_in, query_wide, key_wide, value_wide, query_narrow, key_narrow, value_narrow,
    decay_wide, decay_narrow, gain_wide, gain_narrow, out_wide, out_narrow, mlp_gain,
    up_weight, down_weight,
):
    members = lax.axis_size("tp")
    length, width = stream_in.shape
    portion = length // members
    member = lax.axis_index("tp")
    place = jnp.stack([lax.axis_index("core"), lax.axis_index("zb")]).astype(jnp.int32)

    both = jnp.concatenate([up_weight, down_weight.T], axis=1)
    weights = lax.all_gather(both, SP, axis=0, tiled=True)

    wide_key, wide_value = key_wide.shape[1], value_wide.shape[1]
    thin_value = value_narrow.shape[1]
    half = wide_key // 2
    lanes = wide_value + 2 * LANES
    own = call(
        own_state, shaped((2, half, lanes), BF16),
        key_wide, value_wide, decay_wide, key_narrow, value_narrow, decay_narrow,
        flops=2 * length * wide_key * wide_value, moved=10**6,
    )
    sibling = swap(own)
    within = call(
        inside, shaped((length, wide_value + thin_value), F32),
        query_wide, key_wide, value_wide, decay_wide,
        query_narrow, key_narrow, value_narrow, decay_narrow,
        flops=6 * length * length * wide_value, moved=4 * 10**6,
    )
    rows = half // 4
    pieces = call(of_chip, shaped((4, rows, lanes), BF16), place, own, sibling)
    got = among([pieces[d] for d in range(4)])
    total = call(
        of_group, shaped((1, rows, lanes), BF16), place, *got,
        scratch=[pltpu.VMEM((4, rows, lanes), BF16)],
    )
    size = lax.axis_size("za")
    near, mid, far = [shift(total, "za", d, size, wrap=False) for d in range(1, 4)]
    found = call(
        before_each, shaped((4, rows, lanes - LANES), BF16), place, *got, near, mid, far,
        scratch=[pltpu.VMEM((4, rows, lanes), BF16), pltpu.VMEM((4, rows, lanes - LANES), BF16)],
    )
    back = among([found[d] for d in range(4)])
    own_half = call(gathered_half, shaped((half, lanes - LANES), BF16), place, *back)
    other_half = swap(own_half)
    partial = call(
        heads_out, shaped((length, width), BF16),
        place, own_half, other_half, sibling, query_wide, query_narrow,
        decay_wide, decay_narrow, within, gain_wide[None], gain_narrow[None],
        out_wide, out_narrow,
        scratch=[
            pltpu.VMEM((wide_key, wide_value), BF16),
            pltpu.VMEM((key_narrow.shape[1], thin_value), BF16),
        ],
        flops=4 * length * wide_value * width, moved=8 * 10**6,
    )
    parts = lax.all_to_all(partial.reshape(members, portion, width), "tp", 0, 0, tiled=True)
    own_stream = lax.dynamic_slice_in_dim(stream_in, member * portion, portion, 0)
    middle, normed = call(
        rows_mid, [shaped((portion, width), BF16)] * 2, parts, own_stream, mlp_gain[None]
    )
    copies = jnp.broadcast_to(normed[None], (members, portion, width))
    everyone = lax.all_to_all(copies, "tp", 0, 0, tiled=True).reshape(length, width)
    units = up_weight.shape[1]
    raised = jax.nn.relu(jnp.dot(everyone, weights[:, :units], preferred_element_type=F32))
    hidden = (raised * raised).astype(BF16)
    channel = lax.dot_general(
        hidden, weights[:, units:], (((1,), (1,)), ((), ())), preferred_element_type=F32
    ).astype(BF16)
    summed = lax.all_to_all(channel.reshape(members, portion, width), "tp", 0, 0, tiled=True)
    return (middle.astype(F32) + summed.astype(F32).sum(axis=0)).astype(BF16)


def solution(mesh):
    grp, sp, tp = mesh.shape["grp"], mesh.shape["sp"], mesh.shape["tp"]
    torus = Mesh(
        mesh.devices.reshape(grp, sp // 8, 4, 2, tp), ("grp", "za", "zb", "core", "tp")
    )
    placed = (
        P(GRP_SP, None),
        P(GRP_SP, "tp"),
        P(GRP_SP, "tp"),
        P(GRP_SP, "tp"),
        P(GRP_SP, "tp"),
        P(GRP_SP, "tp"),
        P(GRP_SP, "tp"),
        P("tp", GRP_SP),
        P("tp", GRP_SP),
        P("tp"),
        P("tp"),
        P("tp", None),
        P("tp", None),
        P(),
        P(SP, "tp"),
        P("tp", SP),
    )
    return jax.shard_map(
        on_device, mesh=torus, in_specs=placed, out_specs=P(GRP_SP_TP, None), check_vma=False
    )
```

```python
import jax
import jax.numpy as jnp
from jax import lax
from jax.experimental import pallas as pl
from jax.experimental.pallas import tpu as pltpu
from jax.sharding import Mesh
from jax.sharding import PartitionSpec as P

EPS = 1e-06
SP = ("za", "zb", "core")
GRP_SP = ("grp", "za", "zb", "core")
GRP_SP_TP = ("grp", "za", "zb", "core", "tp")
F32 = jnp.float32
BF16 = jnp.bfloat16
LANES = 128


def vmem():
    return pl.BlockSpec(memory_space=pltpu.VMEM)


def smem():
    return pl.BlockSpec(memory_space=pltpu.SMEM)


def whole(a):
    return pl.BlockSpec(a.shape, lambda *_: (0,) * len(a.shape))


def call(body, outs, *args, scratch=(), flops=0, moved=0, pull=False):
    many = isinstance(outs, (list, tuple))
    outs = list(outs) if many else [outs]
    inner, pulled = body, []
    if pull:
        pulled = [n for n, a in enumerate(args) if a.dtype != jnp.int32]

        def inner(*refs):
            given = list(refs[: len(args)])
            kept = refs[len(args) : len(refs) - len(pulled) - 1]
            held, sems = refs[len(refs) - len(pulled) - 1 : -1], refs[-1]
            copies = []
            for k, n in enumerate(pulled):
                copies.append(pltpu.make_async_copy(given[n], held[k], sems.at[k]))
                copies[-1].start()
                given[n] = held[k]
            for copy in copies:
                copy.wait()
            body(*given, *kept)

        far = pl.BlockSpec(memory_space=pltpu.HBM)
        specs = [smem() if a.dtype == jnp.int32 else far for a in args]
        scratch = list(scratch) + [pltpu.VMEM(args[n].shape, args[n].dtype) for n in pulled]
        scratch.append(pltpu.SemaphoreType.DMA((len(pulled),)))
    else:
        specs = [smem() if a.dtype == jnp.int32 else vmem() for a in args]
    result = pl.pallas_call(
        inner,
        grid=(1,) if pull else (),
        out_shape=outs,
        in_specs=specs,
        out_specs=[whole(o) if pull else vmem() for o in outs],
        scratch_shapes=list(scratch),
        compiler_params=pltpu.CompilerParams(vmem_limit_bytes=48 * 2**20),
        cost_estimate=pl.CostEstimate(flops=flops, bytes_accessed=moved, transcendentals=0),
        name=body.__name__,
    )(*args)
    return result if many else result[0]


def shaped(shape, dtype):
    return jax.ShapeDtypeStruct(shape, dtype)


def mm(a, b, dims=((1,), (0,))):
    return lax.dot_general(a, b, (dims, ((), ())), preferred_element_type=F32)


def three(x):
    high = x.astype(BF16).astype(F32)
    mid = (x - high).astype(BF16).astype(F32)
    low = (x - high - mid).astype(BF16).astype(F32)
    return high, mid, low


def pick(index, values):
    out = jnp.zeros_like(index, dtype=F32)
    for n, value in enumerate(values):
        out = jnp.where(index == n, value, out)
    return out


def decay_rows(dw, dn):
    row = lax.broadcasted_iota(jnp.int32, (8, dw.shape[1]), 0)
    return pick(row, three(dw) + three(dn)).astype(BF16)


def columns(table):
    wide = table[:, 0:1] + table[:, 1:2] + table[:, 2:3]
    thin = table[:, 3:4] + table[:, 4:5] + table[:, 5:6]
    return wide, thin


def log_lanes(wide, thin, rows):
    lane = lax.broadcasted_iota(jnp.int32, (rows, LANES), 1)
    return pick(lane, three(wide) + three(thin))


def positions(length):
    row = lax.broadcasted_iota(jnp.int32, (length, length), 0)
    col = lax.broadcasted_iota(jnp.int32, (length, length), 1)
    return row, col


def own_state(kw, vw, dw, kn, vn, dn, out):
    length = kw.shape[0]
    row, col = positions(length)
    later = (col > row).astype(F32).astype(BF16)
    table = decay_rows(dw[...], dn[...])
    end_wide, end_thin = columns(mm(later, table, ((1,), (1,))))
    total_wide = jnp.sum(dw[...], axis=1, keepdims=True)
    total_thin = jnp.sum(dn[...], axis=1, keepdims=True)

    def state(k, v, end):
        keyed = k[...].astype(F32) * k.shape[1] ** (-0.5) * jnp.exp(end)
        return mm(keyed.astype(BF16), v[...], ((0,), (0,))).astype(BF16)

    wide = state(kw, vw, end_wide)
    thin = state(kn, vn, end_thin)
    half_wide, half_thin = wide.shape[0] // 2, thin.shape[0] // 2
    at = wide.shape[1]
    logs = log_lanes(total_wide, total_thin, half_wide).astype(BF16)
    for h in range(2):
        out[h, :, :at] = wide[h * half_wide : (h + 1) * half_wide]
        part = thin[h * half_thin : (h + 1) * half_thin]
        out[h, :half_thin, at : at + LANES] = part[:, :LANES]
        out[h, half_thin:, at : at + LANES] = part[:, LANES:]
        out[h, :, at + LANES :] = logs


def inside(qw, kw, vw, dw, qn, kn, vn, dn, out):
    length = kw.shape[0]
    row, col = positions(length)
    causal = row >= col
    upto = causal.astype(F32).astype(BF16)
    table = decay_rows(dw[...], dn[...])
    col_wide, col_thin = columns(mm(upto, table, ((1,), (1,))))
    rows = mm(table, upto, ((1,), (1,)))
    row_wide = rows[0:1] + rows[1:2] + rows[2:3]
    row_thin = rows[3:4] + rows[4:5] + rows[5:6]

    def within(q, k, v, by_col, by_row):
        gap = jnp.where(causal, by_col - by_row, 0.0)
        fading = jnp.where(causal, jnp.exp(gap), 0.0)
        weights = mm(q[...], k[...], ((1,), (1,))) * k.shape[1] ** (-0.5) * fading
        return mm(weights.astype(BF16), v[...])

    at = vw.shape[1]
    out[:, :at] = within(qw, kw, vw, col_wide, row_wide)
    out[:, at:] = within(qn, kn, vn, col_thin, row_thin)


def unpack(x):
    x = x.astype(F32)
    cut = x.shape[-1] - LANES
    wide, thin = columns(x[:, cut:])
    return x[:, : cut - LANES], x[:, cut - LANES : cut], wide, thin


def after(earlier, latter):
    return (
        jnp.exp(latter[2]) * earlier[0] + latter[0],
        jnp.exp(latter[3]) * earlier[1] + latter[1],
        earlier[2] + latter[2],
        earlier[3] + latter[3],
    )


def put(ref, at, state, logs=True):
    rows, wide, thin = state[0].shape[0], state[0].shape[1], state[1].shape[1]
    ref[at, :, :wide] = state[0].astype(BF16)
    ref[at, :, wide : wide + thin] = state[1].astype(BF16)
    if logs:
        ref[at, :, wide + thin :] = log_lanes(state[2], state[3], rows).astype(BF16)


def of_chip(place, own, sibling, out):
    core, spot = place[0], place[1]
    first_core = core == 0
    pieces, rows = out.shape[0], out.shape[1]
    for d in range(pieces):
        start = pl.multiple_of(lax.rem(spot + d, pieces) * rows, rows)
        mine = own[core, pl.ds(start, rows), :]
        other = sibling[core, pl.ds(start, rows), :]
        first = jnp.where(first_core, mine, other)
        second = jnp.where(first_core, other, mine)
        put(out, d, after(unpack(first), unpack(second)))


def in_order(place, parts, ordered):
    pieces = len(parts)
    for d, part in enumerate(parts):
        ordered[lax.rem(place[1] - d + pieces, pieces)] = part[...]


def of_group(place, a, b, c, d, out, ordered):
    in_order(place, (a, b, c, d), ordered)
    total = unpack(ordered[0])
    for n in range(1, 4):
        total = after(total, unpack(ordered[n]))
    put(out, 0, total)


def before_each(place, a, b, c, d, near, mid, far, out, ordered, found):
    in_order(place, (a, b, c, d), ordered)
    state = after(after(unpack(far[0]), unpack(mid[0])), unpack(near[0]))
    for n in range(4):
        put(found, n, state, logs=False)
        state = after(state, unpack(ordered[n]))
    for n in range(4):
        out[n] = found[lax.rem(place[1] + n, 4)]


def gathered_half(place, a, b, c, d, out):
    parts = (a, b, c, d)
    rows = a.shape[0]
    for n, part in enumerate(parts):
        start = pl.multiple_of(lax.rem(place[1] - n + 4, 4) * rows, rows)
        out[pl.ds(start, rows), :] = part[...]


def heads_out(
    place, own_half, other_half, sibling, qw, qn, dw, dn, within, gw, gn, ow, on,
    far_a, far_b, right_a, right_b, left_a, left_b, own_a, own_b,
    came_wide, came_thin, turned_wide, turned_thin,
):
    first_core = place[0] == 0
    length = qw.shape[0]
    wide_width, thin_width = gw.shape[1], gn.shape[1]
    half_thin = came_thin.shape[0] // 2
    rows = own_half.shape[0]
    for h in range(2):
        mine = own_half[...] if h == 0 else other_half[...]
        other = other_half[...] if h == 0 else own_half[...]
        before = jnp.where(first_core, mine, other).astype(F32)
        s_wide, s_thin, l_wide, l_thin = unpack(sibling[h])
        b_wide, b_thin = before[:, :wide_width], before[:, wide_width:]
        wide = jnp.where(first_core, b_wide, jnp.exp(l_wide) * b_wide + s_wide)
        thin = jnp.where(first_core, b_thin, jnp.exp(l_thin) * b_thin + s_thin)
        came_wide[h * rows : (h + 1) * rows, :] = wide.astype(BF16)
        low = thin.astype(BF16)
        came_thin[h * half_thin : (h + 1) * half_thin, :LANES] = low[:half_thin]
        came_thin[h * half_thin : (h + 1) * half_thin, LANES:] = low[half_thin:]
    row, col = positions(length)
    upto = (row >= col).astype(F32).astype(BF16)
    cum_wide, cum_thin = columns(mm(upto, decay_rows(dw[...], dn[...]), ((1,), (1,))))

    def normed(q, came, cum, inner, gain):
        kept = inner + mm(q[...], came[...]) * jnp.exp(cum)
        centered = kept - jnp.mean(kept, axis=-1, keepdims=True)
        power = jnp.mean(centered * centered, axis=-1, keepdims=True)
        return (centered * lax.rsqrt(power + EPS) * gain[...]).astype(BF16)

    wide = normed(qw, came_wide, cum_wide, within[:, :wide_width], gw)
    thin = normed(qn, came_thin, cum_thin, within[:, wide_width:], gn)
    outs = (far_a, far_b, right_a, right_b, left_a, left_b, own_a, own_b)
    rows, members = far_a.shape[0], length // (2 * far_a.shape[0])
    for m in range(members):
        spot = lax.rem(m - place[2] + members, members)
        order = jnp.where(spot == 2, 0, jnp.where(spot == 1, 1, jnp.where(spot == 3, 2, 3)))
        start = pl.multiple_of(order * 2 * rows, 2 * rows)
        turned_wide[pl.ds(start, 2 * rows), :] = wide[m * 2 * rows : (m + 1) * 2 * rows]
        turned_thin[pl.ds(start, 2 * rows), :] = thin[m * 2 * rows : (m + 1) * 2 * rows]
    step = 512
    for n in range(ow.shape[1] // step):
        cols = slice(n * step, (n + 1) * step)
        done = (mm(turned_wide[...], ow[:, cols]) + mm(turned_thin[...], on[:, cols])).astype(BF16)
        for m, out in enumerate(outs):
            out[:, cols] = done[m * rows : (m + 1) * rows]


def add_two(a, b, c, d, first, second):
    first[...] = (a[...].astype(F32) + b[...].astype(F32)).astype(BF16)
    second[...] = (c[...].astype(F32) + d[...].astype(F32)).astype(BF16)


def rows_mid(
    own_a, left_a, right_a, own_b, left_b, right_b, stream, gain,
    mid_a, mid_b, normed_a, normed_b,
):
    rows = own_a.shape[0]
    halves = ((own_a, left_a, right_a, mid_a, normed_a), (own_b, left_b, right_b, mid_b, normed_b))
    for n, (own, left, right, middle, normed) in enumerate(halves):
        total = own[...].astype(F32) + left[...].astype(F32) + right[...].astype(F32)
        mid = (stream[n * rows : (n + 1) * rows].astype(F32) + total).astype(BF16)
        middle[...] = mid
        values = mid.astype(F32)
        power = jnp.mean(values * values, axis=-1, keepdims=True)
        normed[...] = (values * lax.rsqrt(power + EPS) * gain[...]).astype(BF16)


def hidden_rows(a, b, c, d, up, down, out_a, out_b, out_c, out_d, rows, hidden, sems):
    step = pl.program_id(0)
    size, block = a.shape[0], up.shape[1]
    ups = hidden.shape[1] // block

    @pl.when(step == 0)
    def _():
        copies = [
            pltpu.make_async_copy(part, rows.at[pl.ds(n * size, size), :], sems.at[n])
            for n, part in enumerate((a, b, c, d))
        ]
        for copy in copies:
            copy.start()
        for copy in copies:
            copy.wait()

    @pl.when(step < ups)
    def _():
        raised = jnp.maximum(mm(rows[...], up[...]), 0.0)
        start = pl.multiple_of(step * block, block)
        hidden[:, pl.ds(start, block)] = (raised * raised).astype(BF16)

    @pl.when(step >= ups)
    def _():
        done = mm(hidden[...], down[...], ((1,), (1,))).astype(BF16)
        for n, out in enumerate((out_a, out_b, out_c, out_d)):
            out[...] = done[n * size : (n + 1) * size]


def feed_forward(parts, weights):
    size, width = parts[0].shape
    units = weights.shape[1] // 2
    block = 256
    ups, downs = units // block, width // block
    put_out = pl.BlockSpec((size, block), lambda s: (0, jnp.maximum(s - ups, 0)))
    return pl.pallas_call(
        hidden_rows,
        grid=(ups + downs,),
        out_shape=[shaped((size, width), BF16)] * 4,
        in_specs=[pl.BlockSpec(memory_space=pltpu.HBM) for _ in parts]
        + [
            pl.BlockSpec((width, block), lambda s: (0, jnp.minimum(s, ups - 1))),
            pl.BlockSpec((block, units), lambda s: (jnp.maximum(s - ups, 0), 1)),
        ],
        out_specs=[put_out] * 4,
        scratch_shapes=[
            pltpu.VMEM((4 * size, width), BF16),
            pltpu.VMEM((4 * size, units), BF16),
            pltpu.SemaphoreType.DMA((4,)),
        ],
        compiler_params=pltpu.CompilerParams(vmem_limit_bytes=48 * 2**20),
        cost_estimate=pl.CostEstimate(
            flops=16 * size * width * units, bytes_accessed=4 * units * width, transcendentals=0
        ),
        name="hidden_rows",
    )(*parts, weights, weights)


def last_sum(own_a, left_a, right_a, mid_a, own_b, left_b, right_b, mid_b, out):
    rows = own_a.shape[0]
    halves = ((own_a, left_a, right_a, mid_a), (own_b, left_b, right_b, mid_b))
    for n, parts in enumerate(halves):
        total = parts[3][...].astype(F32)
        for part in parts[:3]:
            total = total + part[...].astype(F32)
        out[n * rows : (n + 1) * rows] = total.astype(BF16)


def shift(x, axis, by, size, wrap=True):
    pairs = [(i, (i + by) % size) for i in range(size) if wrap or 0 <= i + by < size]
    return lax.ppermute(x, axis, pairs)


def swap(x):
    return lax.ppermute(x, "core", [(0, 1), (1, 0)])


def turn(x, by):
    return shift(x, "tp", by, lax.axis_size("tp"))


def sent_far(far_a, far_b):
    return turn(far_a, 1), turn(far_b, -1)


def reduced(far, right_a, right_b, left_a, left_b):
    came_right_b, came_left_a = turn(right_b, 1), turn(left_a, -1)
    like = [shaped(right_a.shape, BF16)] * 2
    right_sum, left_sum = call(add_two, like, right_a, far[0], left_b, far[1], pull=True)
    return turn(right_sum, 1), came_right_b, came_left_a, turn(left_sum, -1)


def spread(a, b):
    left_a, right_b = turn(a, 1), turn(b, -1)
    left_b, right_a = turn(b, 1), turn(a, -1)
    far_a, far_b = turn(left_a, 1), turn(right_b, -1)
    return far_a, far_b, right_a, right_b, left_a, left_b


def among(parts):
    return [parts[0]] + [shift(parts[d], "zb", d, 4) for d in range(1, 4)]


def on_device(
    stream_in, query_wide, key_wide, value_wide, query_narrow, key_narrow, value_narrow,
    decay_wide, decay_narrow, gain_wide, gain_narrow, out_wide, out_narrow, mlp_gain,
    up_weight, down_weight,
):
    members = lax.axis_size("tp")
    length, width = stream_in.shape
    portion = length // members
    member = lax.axis_index("tp")
    place = jnp.stack([lax.axis_index(n) for n in ("core", "zb", "tp")]).astype(jnp.int32)

    both = jnp.concatenate([up_weight, down_weight.T], axis=1)
    weights = lax.all_gather(both, SP, axis=0, tiled=True)

    wide_key, wide_value = key_wide.shape[1], value_wide.shape[1]
    thin_value = value_narrow.shape[1]
    half = wide_key // 2
    lanes = wide_value + 2 * LANES
    own = call(
        own_state, shaped((2, half, lanes), BF16),
        key_wide, value_wide, decay_wide, key_narrow, value_narrow, decay_narrow,
        flops=2 * length * wide_key * wide_value, moved=10**6, pull=True,
    )
    sibling = swap(own)
    within = call(
        inside, shaped((length, wide_value + thin_value), F32),
        query_wide, key_wide, value_wide, decay_wide,
        query_narrow, key_narrow, value_narrow, decay_narrow,
        flops=6 * length * length * wide_value, moved=4 * 10**6, pull=True,
    )
    rows = half // 4
    pieces = call(of_chip, shaped((4, rows, lanes), BF16), place, own, sibling)
    got = among([pieces[d] for d in range(4)])
    total = call(
        of_group, shaped((1, rows, lanes), BF16), place, *got,
        scratch=[pltpu.VMEM((4, rows, lanes), BF16)],
    )
    size = lax.axis_size("za")
    near, mid, far = [shift(total, "za", d, size, wrap=False) for d in range(1, 4)]
    found = call(
        before_each, shaped((4, rows, lanes - LANES), BF16), place, *got, near, mid, far,
        scratch=[pltpu.VMEM((4, rows, lanes), BF16), pltpu.VMEM((4, rows, lanes - LANES), BF16)],
    )
    back = among([found[d] for d in range(4)])
    own_half = call(gathered_half, shaped((half, lanes - LANES), BF16), place, *back)
    other_half = swap(own_half)
    quarter = portion // 2
    far_a, far_b, right_a, right_b, left_a, left_b, own_a, own_b = call(
        heads_out, [shaped((quarter, width), BF16)] * 8,
        place, own_half, other_half, sibling, query_wide, query_narrow,
        decay_wide, decay_narrow, within, gain_wide[None], gain_narrow[None],
        out_wide, out_narrow,
        scratch=[
            pltpu.VMEM((wide_key, wide_value), BF16),
            pltpu.VMEM((key_narrow.shape[1], thin_value), BF16),
            pltpu.VMEM((length, wide_value), BF16),
            pltpu.VMEM((length, thin_value), BF16),
        ],
        flops=4 * length * wide_value * width, moved=8 * 10**6, pull=True,
    )
    from_left_a, from_left_b, from_right_a, from_right_b = reduced(
        sent_far(far_a, far_b), right_a, right_b, left_a, left_b
    )
    own_stream = lax.dynamic_slice_in_dim(stream_in, member * portion, portion, 0)
    mid_a, mid_b, normed_a, normed_b = call(
        rows_mid, [shaped((quarter, width), BF16)] * 4,
        own_a, from_left_a, from_right_a, own_b, from_left_b, from_right_b,
        own_stream, mlp_gain[None], pull=True,
    )
    far_a, far_b, right_a, right_b, left_a, left_b = spread(normed_a, normed_b)
    far_a, far_b, right_a, right_b = feed_forward((far_a, far_b, right_a, right_b), weights)
    far = sent_far(far_a, far_b)
    left_a, left_b, own_a, own_b = feed_forward((left_a, left_b, normed_a, normed_b), weights)
    from_left_a, from_left_b, from_right_a, from_right_b = reduced(
        far, right_a, right_b, left_a, left_b
    )
    return call(
        last_sum, shaped((portion, width), BF16),
        own_a, from_left_a, from_right_a, mid_a, own_b, from_left_b, from_right_b, mid_b, pull=True,
    )


def solution(mesh):
    grp, sp, tp = mesh.shape["grp"], mesh.shape["sp"], mesh.shape["tp"]
    torus = Mesh(
        mesh.devices.reshape(grp, sp // 8, 4, 2, tp), ("grp", "za", "zb", "core", "tp")
    )
    placed = (
        P(GRP_SP, None),
        P(GRP_SP, "tp"),
        P(GRP_SP, "tp"),
        P(GRP_SP, "tp"),
        P(GRP_SP, "tp"),
        P(GRP_SP, "tp"),
        P(GRP_SP, "tp"),
        P("tp", GRP_SP),
        P("tp", GRP_SP),
        P("tp"),
        P("tp"),
        P("tp", None),
        P("tp", None),
        P(),
        P(SP, "tp"),
        P("tp", SP),
    )
    return jax.shard_map(
        on_device, mesh=torus, in_specs=placed, out_specs=P(GRP_SP_TP, None), check_vma=False
    )
```

```python
import jax
import jax.numpy as jnp
from jax import lax
from jax.experimental import pallas as pl
from jax.experimental.pallas import tpu as pltpu
from jax.sharding import Mesh
from jax.sharding import PartitionSpec as P

EPS = 1e-06
SP = ("za", "zb", "core")
GRP_SP = ("grp", "za", "zb", "core")
GRP_SP_TP = ("grp", "za", "zb", "core", "tp")
F32 = jnp.float32
BF16 = jnp.bfloat16
LANES = 128


def vmem():
    return pl.BlockSpec(memory_space=pltpu.VMEM)


def smem():
    return pl.BlockSpec(memory_space=pltpu.SMEM)


class Far:
    def __init__(self, x):
        self.x = x


def call(body, outs, *args, scratch=(), flops=0, moved=0, far_out=False, limit=48):
    many = isinstance(outs, (list, tuple))
    outs = list(outs) if many else [outs]
    pulled = [n for n, a in enumerate(args) if isinstance(a, Far)]
    args = [
        pltpu.with_memory_space_constraint(a.x, pltpu.HBM) if isinstance(a, Far) else a
        for a in args
    ]
    pushed = list(range(len(outs))) if far_out else []
    own = len(scratch)

    def inner(*refs):
        given, rest = list(refs[: len(args)]), list(refs[len(args) :])
        results, rest = rest[: len(outs)], rest[len(outs) :]
        kept, rest = rest[:own], rest[own:]
        held, sent = rest[: len(pulled)], rest[len(pulled) : len(pulled) + len(pushed)]
        sems = rest[-1]
        copies = []
        for k, n in enumerate(pulled):
            copies.append(pltpu.make_async_copy(given[n], held[k], sems.at[k]))
            copies[-1].start()
            given[n] = held[k]
        for copy in copies:
            copy.wait()
        body(*given, *(sent if pushed else results), *kept)
        copies = []
        for k in range(len(pushed)):
            copies.append(pltpu.make_async_copy(sent[k], results[k], sems.at[len(pulled) + k]))
            copies[-1].start()
        for copy in copies:
            copy.wait()

    far = pl.BlockSpec(memory_space=pltpu.HBM)
    specs = [
        smem() if a.dtype == jnp.int32 else far if n in pulled else vmem()
        for n, a in enumerate(args)
    ]
    buffers = [pltpu.VMEM(args[n].shape, args[n].dtype) for n in pulled]
    buffers += [pltpu.VMEM(outs[n].shape, outs[n].dtype) for n in pushed]
    result = pl.pallas_call(
        inner,
        out_shape=[pltpu.HBM(o.shape, o.dtype) for o in outs] if far_out else outs,
        in_specs=specs,
        out_specs=[far if far_out else vmem() for _ in outs],
        scratch_shapes=[
            *scratch, *buffers, pltpu.SemaphoreType.DMA((max(len(pulled) + len(pushed), 1),))
        ],
        compiler_params=pltpu.CompilerParams(vmem_limit_bytes=limit * 2**20),
        cost_estimate=pl.CostEstimate(flops=flops, bytes_accessed=moved, transcendentals=0),
        name=body.__name__,
    )(*args)
    return result if many else result[0]


def shaped(shape, dtype):
    return jax.ShapeDtypeStruct(shape, dtype)


def mm(a, b, dims=((1,), (0,))):
    return lax.dot_general(a, b, (dims, ((), ())), preferred_element_type=F32)


def three(x):
    high = x.astype(BF16).astype(F32)
    mid = (x - high).astype(BF16).astype(F32)
    low = (x - high - mid).astype(BF16).astype(F32)
    return high, mid, low


def pick(index, values):
    out = jnp.zeros_like(index, dtype=F32)
    for n, value in enumerate(values):
        out = jnp.where(index == n, value, out)
    return out


def decay_rows(dw, dn):
    row = lax.broadcasted_iota(jnp.int32, (8, dw.shape[1]), 0)
    return pick(row, three(dw) + three(dn)).astype(BF16)


def columns(table):
    wide = table[:, 0:1] + table[:, 1:2] + table[:, 2:3]
    thin = table[:, 3:4] + table[:, 4:5] + table[:, 5:6]
    return wide, thin


def log_lanes(wide, thin, rows):
    lane = lax.broadcasted_iota(jnp.int32, (rows, LANES), 1)
    return pick(lane, three(wide) + three(thin))


def positions(length):
    row = lax.broadcasted_iota(jnp.int32, (length, length), 0)
    col = lax.broadcasted_iota(jnp.int32, (length, length), 1)
    return row, col


def own_state(kw, vw, dw, kn, vn, dn, out):
    length = kw.shape[0]
    row, col = positions(length)
    later = (col > row).astype(F32).astype(BF16)
    table = decay_rows(dw[...], dn[...])
    end_wide, end_thin = columns(mm(later, table, ((1,), (1,))))
    total_wide = jnp.sum(dw[...], axis=1, keepdims=True)
    total_thin = jnp.sum(dn[...], axis=1, keepdims=True)

    def state(k, v, end):
        keyed = k[...].astype(F32) * k.shape[1] ** (-0.5) * jnp.exp(end)
        return mm(keyed.astype(BF16), v[...], ((0,), (0,))).astype(BF16)

    wide = state(kw, vw, end_wide)
    thin = state(kn, vn, end_thin)
    half_wide, half_thin = wide.shape[0] // 2, thin.shape[0] // 2
    at = wide.shape[1]
    logs = log_lanes(total_wide, total_thin, half_wide).astype(BF16)
    for h in range(2):
        out[h, :, :at] = wide[h * half_wide : (h + 1) * half_wide]
        part = thin[h * half_thin : (h + 1) * half_thin]
        out[h, :half_thin, at : at + LANES] = part[:, :LANES]
        out[h, half_thin:, at : at + LANES] = part[:, LANES:]
        out[h, :, at + LANES :] = logs


def inside(qw, kw, vw, dw, qn, kn, vn, dn, out):
    length = kw.shape[0]
    row, col = positions(length)
    causal = row >= col
    upto = causal.astype(F32).astype(BF16)
    table = decay_rows(dw[...], dn[...])
    col_wide, col_thin = columns(mm(upto, table, ((1,), (1,))))
    rows = mm(table, upto, ((1,), (1,)))
    row_wide = rows[0:1] + rows[1:2] + rows[2:3]
    row_thin = rows[3:4] + rows[4:5] + rows[5:6]

    def within(q, k, v, by_col, by_row):
        gap = jnp.where(causal, by_col - by_row, 0.0)
        fading = jnp.where(causal, jnp.exp(gap), 0.0)
        weights = mm(q[...], k[...], ((1,), (1,))) * k.shape[1] ** (-0.5) * fading
        return mm(weights.astype(BF16), v[...])

    at = vw.shape[1]
    out[:, :at] = within(qw, kw, vw, col_wide, row_wide)
    out[:, at:] = within(qn, kn, vn, col_thin, row_thin)


def unpack(x):
    x = x.astype(F32)
    cut = x.shape[-1] - LANES
    wide, thin = columns(x[:, cut:])
    return x[:, : cut - LANES], x[:, cut - LANES : cut], wide, thin


def after(earlier, latter):
    return (
        jnp.exp(latter[2]) * earlier[0] + latter[0],
        jnp.exp(latter[3]) * earlier[1] + latter[1],
        earlier[2] + latter[2],
        earlier[3] + latter[3],
    )


def put(ref, at, state, logs=True):
    rows, wide, thin = state[0].shape[0], state[0].shape[1], state[1].shape[1]
    ref[at, :, :wide] = state[0].astype(BF16)
    ref[at, :, wide : wide + thin] = state[1].astype(BF16)
    if logs:
        ref[at, :, wide + thin :] = log_lanes(state[2], state[3], rows).astype(BF16)


def of_chip(place, own, sibling, out):
    core, spot = place[0], place[1]
    first_core = core == 0
    pieces, rows = out.shape[0], out.shape[1]
    for d in range(pieces):
        start = pl.multiple_of(lax.rem(spot + d, pieces) * rows, rows)
        mine = own[core, pl.ds(start, rows), :]
        other = sibling[core, pl.ds(start, rows), :]
        first = jnp.where(first_core, mine, other)
        second = jnp.where(first_core, other, mine)
        put(out, d, after(unpack(first), unpack(second)))


def in_order(place, parts, ordered):
    pieces = len(parts)
    for d, part in enumerate(parts):
        ordered[lax.rem(place[1] - d + pieces, pieces)] = part[...]


def of_group(place, a, b, c, d, out, ordered):
    in_order(place, (a, b, c, d), ordered)
    total = unpack(ordered[0])
    for n in range(1, 4):
        total = after(total, unpack(ordered[n]))
    put(out, 0, total)


def before_each(place, a, b, c, d, near, mid, far, out, ordered, found):
    in_order(place, (a, b, c, d), ordered)
    state = after(after(unpack(far[0]), unpack(mid[0])), unpack(near[0]))
    for n in range(4):
        put(found, n, state, logs=False)
        state = after(state, unpack(ordered[n]))
    for n in range(4):
        out[n] = found[lax.rem(place[1] + n, 4)]


def gathered_half(place, a, b, c, d, out):
    parts = (a, b, c, d)
    rows = a.shape[0]
    for n, part in enumerate(parts):
        start = pl.multiple_of(lax.rem(place[1] - n + 4, 4) * rows, rows)
        out[pl.ds(start, rows), :] = part[...]


def heads_out(
    place, own_half, other_half, sibling, qw, qn, dw, dn, within, gw, gn, ow, on,
    far_a, far_b, right_a, right_b, left_a, left_b, own_a, own_b,
    came_wide, came_thin, turned_wide, turned_thin,
):
    first_core = place[0] == 0
    length = qw.shape[0]
    wide_width, thin_width = gw.shape[1], gn.shape[1]
    half_thin = came_thin.shape[0] // 2
    rows = own_half.shape[0]
    for h in range(2):
        mine = own_half[...] if h == 0 else other_half[...]
        other = other_half[...] if h == 0 else own_half[...]
        before = jnp.where(first_core, mine, other).astype(F32)
        s_wide, s_thin, l_wide, l_thin = unpack(sibling[h])
        b_wide, b_thin = before[:, :wide_width], before[:, wide_width:]
        wide = jnp.where(first_core, b_wide, jnp.exp(l_wide) * b_wide + s_wide)
        thin = jnp.where(first_core, b_thin, jnp.exp(l_thin) * b_thin + s_thin)
        came_wide[h * rows : (h + 1) * rows, :] = wide.astype(BF16)
        low = thin.astype(BF16)
        came_thin[h * half_thin : (h + 1) * half_thin, :LANES] = low[:half_thin]
        came_thin[h * half_thin : (h + 1) * half_thin, LANES:] = low[half_thin:]
    row, col = positions(length)
    upto = (row >= col).astype(F32).astype(BF16)
    cum_wide, cum_thin = columns(mm(upto, decay_rows(dw[...], dn[...]), ((1,), (1,))))

    def normed(q, came, cum, inner, gain):
        kept = inner + mm(q[...], came[...]) * jnp.exp(cum)
        centered = kept - jnp.mean(kept, axis=-1, keepdims=True)
        power = jnp.mean(centered * centered, axis=-1, keepdims=True)
        return (centered * lax.rsqrt(power + EPS) * gain[...]).astype(BF16)

    wide = normed(qw, came_wide, cum_wide, within[:, :wide_width], gw)
    thin = normed(qn, came_thin, cum_thin, within[:, wide_width:], gn)
    outs = (far_a, far_b, right_a, right_b, left_a, left_b, own_a, own_b)
    rows, members = far_a.shape[0], length // (2 * far_a.shape[0])
    for m in range(members):
        spot = lax.rem(m - place[2] + members, members)
        order = jnp.where(spot == 2, 0, jnp.where(spot == 1, 1, jnp.where(spot == 3, 2, 3)))
        start = pl.multiple_of(order * 2 * rows, 2 * rows)
        turned_wide[pl.ds(start, 2 * rows), :] = wide[m * 2 * rows : (m + 1) * 2 * rows]
        turned_thin[pl.ds(start, 2 * rows), :] = thin[m * 2 * rows : (m + 1) * 2 * rows]
    step = 512
    for n in range(ow.shape[1] // step):
        cols = slice(n * step, (n + 1) * step)
        done = (mm(turned_wide[...], ow[:, cols]) + mm(turned_thin[...], on[:, cols])).astype(BF16)
        for m, out in enumerate(outs):
            out[:, cols] = done[m * rows : (m + 1) * rows]


def add_two(a, b, c, d, first, second):
    first[...] = (a[...].astype(F32) + b[...].astype(F32)).astype(BF16)
    second[...] = (c[...].astype(F32) + d[...].astype(F32)).astype(BF16)


def rows_mid(
    own_a, left_a, right_a, own_b, left_b, right_b, stream, gain,
    mid_a, mid_b, normed_a, normed_b,
):
    rows = own_a.shape[0]
    halves = ((own_a, left_a, right_a, mid_a, normed_a), (own_b, left_b, right_b, mid_b, normed_b))
    for n, (own, left, right, middle, normed) in enumerate(halves):
        total = own[...].astype(F32) + left[...].astype(F32) + right[...].astype(F32)
        mid = (stream[n * rows : (n + 1) * rows].astype(F32) + total).astype(BF16)
        middle[...] = mid
        values = mid.astype(F32)
        power = jnp.mean(values * values, axis=-1, keepdims=True)
        normed[...] = (values * lax.rsqrt(power + EPS) * gain[...]).astype(BF16)


def hidden_rows(
    a, b, c, d, weights, out_a, out_b, out_c, out_d, rows, up, down, total, hidden,
    done_rows, row_sems, up_sems, down_sems, out_sems,
):
    size, block, count = a.shape[0], up.shape[1], up.shape[0]
    units = up.shape[2]
    chunk = rows.shape[2]

    def fetch_rows(n, part, k):
        to = rows.at[k, pl.ds(n * size, size), :]
        return pltpu.make_async_copy(part.at[:, pl.ds(k * chunk, chunk)], to, row_sems.at[n, k])

    def fetch(k, column, to, sems):
        start = pl.multiple_of(k * block, block)
        source = weights.at[pl.ds(start, block), pl.ds(column * units, units)]
        return pltpu.make_async_copy(source, to.at[k], sems.at[k])

    parts = (a, b, c, d)
    for n, part in enumerate(parts):
        for k in range(rows.shape[0]):
            fetch_rows(n, part, k).start()

    @pl.loop(0, count)
    def _(k):
        fetch(k, 0, up, up_sems).start()

    @pl.loop(0, count)
    def _(k):
        fetch(k, 1, down, down_sems).start()

    for n, part in enumerate(parts):
        for k in range(rows.shape[0]):
            fetch_rows(n, part, k).wait()

    total[...] = jnp.zeros_like(total)

    @pl.loop(0, count)
    def _(k):
        fetch(k, 0, up, up_sems).wait()
        total[...] += mm(rows[k], up[k])

    raised = jnp.maximum(total[...], 0.0)
    hidden[...] = (raised * raised).astype(BF16)

    @pl.loop(0, count)
    def _(k):
        fetch(k, 1, down, down_sems).wait()
        done = mm(hidden[...], down[k], ((1,), (1,))).astype(BF16)
        start = pl.multiple_of(k * block, block)
        for n in range(4):
            done_rows[n, :, pl.ds(start, block)] = done[n * size : (n + 1) * size]

    copies = []
    for n, out in enumerate((out_a, out_b, out_c, out_d)):
        copies.append(pltpu.make_async_copy(done_rows.at[n], out, out_sems.at[n]))
        copies[-1].start()
    for copy in copies:
        copy.wait()


def feed_forward(parts, weights):
    size, width = parts[0].shape
    units = weights.shape[1] // 2
    block = 256
    count = width // block
    far = pl.BlockSpec(memory_space=pltpu.HBM)
    held = [pltpu.with_memory_space_constraint(p, pltpu.HBM) for p in (*parts, weights)]
    return pl.pallas_call(
        hidden_rows,
        out_shape=[pltpu.HBM((size, width), BF16)] * 4,
        in_specs=[far] * 5,
        out_specs=[far] * 4,
        scratch_shapes=[
            pltpu.VMEM((count, 4 * size, block), BF16),
            pltpu.VMEM((count, block, units), BF16),
            pltpu.VMEM((count, block, units), BF16),
            pltpu.VMEM((4 * size, units), F32),
            pltpu.VMEM((4 * size, units), BF16),
            pltpu.VMEM((4, size, width), BF16),
            pltpu.SemaphoreType.DMA((4, count)),
            pltpu.SemaphoreType.DMA((count,)),
            pltpu.SemaphoreType.DMA((count,)),
            pltpu.SemaphoreType.DMA((4,)),
        ],
        compiler_params=pltpu.CompilerParams(vmem_limit_bytes=40 * 2**20),
        cost_estimate=pl.CostEstimate(
            flops=16 * size * width * units, bytes_accessed=4 * units * width, transcendentals=0
        ),
        name="hidden_rows",
    )(*held)


def last_sum(own_a, left_a, right_a, mid_a, own_b, left_b, right_b, mid_b, out):
    rows = own_a.shape[0]
    halves = ((own_a, left_a, right_a, mid_a), (own_b, left_b, right_b, mid_b))
    for n, parts in enumerate(halves):
        total = parts[3][...].astype(F32)
        for part in parts[:3]:
            total = total + part[...].astype(F32)
        out[n * rows : (n + 1) * rows] = total.astype(BF16)


def shift(x, axis, by, size, wrap=True):
    pairs = [(i, (i + by) % size) for i in range(size) if wrap or 0 <= i + by < size]
    return lax.ppermute(x, axis, pairs)


def swap(x):
    return lax.ppermute(x, "core", [(0, 1), (1, 0)])


def turn(x, by):
    return shift(x, "tp", by, lax.axis_size("tp"))


def sent_far(far_a, far_b):
    return turn(far_a, 1), turn(far_b, -1)


def reduced(far, right_a, right_b, left_a, left_b):
    came_right_b, came_left_a = turn(right_b, 1), turn(left_a, -1)
    like = [shaped(right_a.shape, BF16)] * 2
    right_sum, left_sum = call(
        add_two, like, Far(right_a), far[0], Far(left_b), far[1], far_out=True, limit=16
    )
    return turn(right_sum, 1), came_right_b, came_left_a, turn(left_sum, -1)


def spread(a, b):
    left_a, right_b = turn(a, 1), turn(b, -1)
    left_b, right_a = turn(b, 1), turn(a, -1)
    far_a, far_b = turn(left_a, 1), turn(right_b, -1)
    return far_a, far_b, right_a, right_b, left_a, left_b


def among(parts):
    return [parts[0]] + [shift(parts[d], "zb", d, 4) for d in range(1, 4)]


def on_device(
    stream_in, query_wide, key_wide, value_wide, query_narrow, key_narrow, value_narrow,
    decay_wide, decay_narrow, gain_wide, gain_narrow, out_wide, out_narrow, mlp_gain,
    up_weight, down_weight,
):
    members = lax.axis_size("tp")
    length, width = stream_in.shape
    portion = length // members
    member = lax.axis_index("tp")
    place = jnp.stack([lax.axis_index(n) for n in ("core", "zb", "tp")]).astype(jnp.int32)

    both = jnp.concatenate([up_weight, down_weight.T], axis=1)
    weights = lax.all_gather(both, SP, axis=0, tiled=True)

    wide_key, wide_value = key_wide.shape[1], value_wide.shape[1]
    thin_value = value_narrow.shape[1]
    half = wide_key // 2
    lanes = wide_value + 2 * LANES
    own = call(
        own_state, shaped((2, half, lanes), BF16),
        *map(Far, (key_wide, value_wide, decay_wide, key_narrow, value_narrow, decay_narrow)),
        flops=2 * length * wide_key * wide_value, moved=10**6,
    )
    sibling = swap(own)
    within = call(
        inside, shaped((length, wide_value + thin_value), F32),
        *map(Far, (query_wide, key_wide, value_wide, decay_wide)),
        *map(Far, (query_narrow, key_narrow, value_narrow, decay_narrow)),
        flops=6 * length * length * wide_value, moved=4 * 10**6,
    )
    rows = half // 4
    pieces = call(of_chip, shaped((4, rows, lanes), BF16), place, own, sibling)
    got = among([pieces[d] for d in range(4)])
    total = call(
        of_group, shaped((1, rows, lanes), BF16), place, *got,
        scratch=[pltpu.VMEM((4, rows, lanes), BF16)],
    )
    size = lax.axis_size("za")
    near, mid, far = [shift(total, "za", d, size, wrap=False) for d in range(1, 4)]
    found = call(
        before_each, shaped((4, rows, lanes - LANES), BF16), place, *got, near, mid, far,
        scratch=[pltpu.VMEM((4, rows, lanes), BF16), pltpu.VMEM((4, rows, lanes - LANES), BF16)],
    )
    back = among([found[d] for d in range(4)])
    own_half = call(gathered_half, shaped((half, lanes - LANES), BF16), place, *back)
    other_half = swap(own_half)
    quarter = portion // 2
    far_a, far_b, right_a, right_b, left_a, left_b, own_a, own_b = call(
        heads_out, [shaped((quarter, width), BF16)] * 8,
        place, own_half, other_half, sibling,
        *map(Far, (query_wide, query_narrow, decay_wide, decay_narrow)), within,
        *map(Far, (gain_wide[None], gain_narrow[None], out_wide, out_narrow)),
        scratch=[
            pltpu.VMEM((wide_key, wide_value), BF16),
            pltpu.VMEM((key_narrow.shape[1], thin_value), BF16),
            pltpu.VMEM((length, wide_value), BF16),
            pltpu.VMEM((length, thin_value), BF16),
        ],
        flops=4 * length * wide_value * width, moved=8 * 10**6, far_out=True,
    )
    from_left_a, from_left_b, from_right_a, from_right_b = reduced(
        sent_far(far_a, far_b), right_a, right_b, left_a, left_b
    )
    own_stream = lax.dynamic_slice_in_dim(stream_in, member * portion, portion, 0)
    mid_a, mid_b, normed_a, normed_b = call(
        rows_mid, [shaped((quarter, width), BF16)] * 4,
        Far(own_a), from_left_a, from_right_a, Far(own_b), from_left_b, from_right_b,
        Far(own_stream), Far(mlp_gain[None]), far_out=True, limit=16,
    )
    far_a, far_b, right_a, right_b, left_a, left_b = spread(normed_a, normed_b)
    far_a, far_b, right_a, right_b = feed_forward((far_a, far_b, right_a, right_b), weights)
    far = sent_far(far_a, far_b)
    left_a, left_b, own_a, own_b = feed_forward((left_a, left_b, normed_a, normed_b), weights)
    from_left_a, from_left_b, from_right_a, from_right_b = reduced(
        far, right_a, right_b, left_a, left_b
    )
    return call(
        last_sum, shaped((portion, width), BF16),
        Far(own_a), from_left_a, from_right_a, Far(mid_a),
        Far(own_b), from_left_b, from_right_b, Far(mid_b), far_out=True, limit=16,
    )


def solution(mesh):
    grp, sp, tp = mesh.shape["grp"], mesh.shape["sp"], mesh.shape["tp"]
    torus = Mesh(
        mesh.devices.reshape(grp, sp // 8, 4, 2, tp), ("grp", "za", "zb", "core", "tp")
    )
    placed = (
        P(GRP_SP, None),
        P(GRP_SP, "tp"),
        P(GRP_SP, "tp"),
        P(GRP_SP, "tp"),
        P(GRP_SP, "tp"),
        P(GRP_SP, "tp"),
        P(GRP_SP, "tp"),
        P("tp", GRP_SP),
        P("tp", GRP_SP),
        P("tp"),
        P("tp"),
        P("tp", None),
        P("tp", None),
        P(),
        P(SP, "tp"),
        P("tp", SP),
    )
    return jax.shard_map(
        on_device, mesh=torus, in_specs=placed, out_specs=P(GRP_SP_TP, None), check_vma=False
    )
```

```python
import jax
import jax.numpy as jnp
from jax import lax
from jax.experimental import pallas as pl
from jax.experimental.pallas import tpu as pltpu
from jax.sharding import Mesh
from jax.sharding import PartitionSpec as P

EPS = 1e-06
SP = ("za", "zb", "core")
GRP_SP = ("grp", "za", "zb", "core")
GRP_SP_TP = ("grp", "za", "zb", "core", "tp")
F32 = jnp.float32
BF16 = jnp.bfloat16
LANES = 128


def vmem():
    return pl.BlockSpec(memory_space=pltpu.VMEM)


def smem():
    return pl.BlockSpec(memory_space=pltpu.SMEM)


class Far:
    def __init__(self, x):
        self.x = x


def call(body, outs, *args, scratch=(), flops=0, moved=0, far_out=False, limit=48):
    many = isinstance(outs, (list, tuple))
    outs = list(outs) if many else [outs]
    pulled = [n for n, a in enumerate(args) if isinstance(a, Far)]
    args = [
        pltpu.with_memory_space_constraint(a.x, pltpu.HBM) if isinstance(a, Far) else a
        for a in args
    ]
    pushed = list(range(len(outs))) if far_out else []
    own = len(scratch)

    def inner(*refs):
        given, rest = list(refs[: len(args)]), list(refs[len(args) :])
        results, rest = rest[: len(outs)], rest[len(outs) :]
        kept, rest = rest[:own], rest[own:]
        held, sent = rest[: len(pulled)], rest[len(pulled) : len(pulled) + len(pushed)]
        sems = rest[-1]
        copies = []
        for k, n in enumerate(pulled):
            copies.append(pltpu.make_async_copy(given[n], held[k], sems.at[k]))
            copies[-1].start()
            given[n] = held[k]
        for copy in copies:
            copy.wait()
        body(*given, *(sent if pushed else results), *kept)
        copies = []
        for k in range(len(pushed)):
            copies.append(pltpu.make_async_copy(sent[k], results[k], sems.at[len(pulled) + k]))
            copies[-1].start()
        for copy in copies:
            copy.wait()

    far = pl.BlockSpec(memory_space=pltpu.HBM)
    specs = [
        smem() if a.dtype == jnp.int32 else far if n in pulled else vmem()
        for n, a in enumerate(args)
    ]
    buffers = [pltpu.VMEM(args[n].shape, args[n].dtype) for n in pulled]
    buffers += [pltpu.VMEM(outs[n].shape, outs[n].dtype) for n in pushed]
    result = pl.pallas_call(
        inner,
        out_shape=[pltpu.HBM(o.shape, o.dtype) for o in outs] if far_out else outs,
        in_specs=specs,
        out_specs=[far if far_out else vmem() for _ in outs],
        scratch_shapes=[
            *scratch, *buffers, pltpu.SemaphoreType.DMA((max(len(pulled) + len(pushed), 1),))
        ],
        compiler_params=pltpu.CompilerParams(vmem_limit_bytes=limit * 2**20),
        cost_estimate=pl.CostEstimate(flops=flops, bytes_accessed=moved, transcendentals=0),
        name=body.__name__,
    )(*args)
    return result if many else result[0]


def shaped(shape, dtype):
    return jax.ShapeDtypeStruct(shape, dtype)


def mm(a, b, dims=((1,), (0,))):
    return lax.dot_general(a, b, (dims, ((), ())), preferred_element_type=F32)


def three(x):
    high = x.astype(BF16).astype(F32)
    mid = (x - high).astype(BF16).astype(F32)
    low = (x - high - mid).astype(BF16).astype(F32)
    return high, mid, low


def pick(index, values):
    out = jnp.zeros_like(index, dtype=F32)
    for n, value in enumerate(values):
        out = jnp.where(index == n, value, out)
    return out


def decay_rows(dw, dn):
    row = lax.broadcasted_iota(jnp.int32, (8, dw.shape[1]), 0)
    return pick(row, three(dw) + three(dn)).astype(BF16)


def columns(table):
    wide = table[:, 0:1] + table[:, 1:2] + table[:, 2:3]
    thin = table[:, 3:4] + table[:, 4:5] + table[:, 5:6]
    return wide, thin


def log_lanes(wide, thin, rows):
    lane = lax.broadcasted_iota(jnp.int32, (rows, LANES), 1)
    return pick(lane, three(wide) + three(thin))


def positions(length):
    row = lax.broadcasted_iota(jnp.int32, (length, length), 0)
    col = lax.broadcasted_iota(jnp.int32, (length, length), 1)
    return row, col


def own_state(kw, vw, dw, kn, vn, dn, out):
    length = kw.shape[0]
    row, col = positions(length)
    later = (col > row).astype(F32).astype(BF16)
    table = decay_rows(dw[...], dn[...])
    end_wide, end_thin = columns(mm(later, table, ((1,), (1,))))
    total_wide = jnp.sum(dw[...], axis=1, keepdims=True)
    total_thin = jnp.sum(dn[...], axis=1, keepdims=True)

    def state(k, v, end):
        keyed = k[...].astype(F32) * k.shape[1] ** (-0.5) * jnp.exp(end)
        return mm(keyed.astype(BF16), v[...], ((0,), (0,))).astype(BF16)

    wide = state(kw, vw, end_wide)
    thin = state(kn, vn, end_thin)
    half_wide, half_thin = wide.shape[0] // 2, thin.shape[0] // 2
    at = wide.shape[1]
    logs = log_lanes(total_wide, total_thin, half_wide).astype(BF16)
    for h in range(2):
        out[h, :, :at] = wide[h * half_wide : (h + 1) * half_wide]
        part = thin[h * half_thin : (h + 1) * half_thin]
        out[h, :half_thin, at : at + LANES] = part[:, :LANES]
        out[h, half_thin:, at : at + LANES] = part[:, LANES:]
        out[h, :, at + LANES :] = logs


def inside(qw, kw, vw, dw, qn, kn, vn, dn, out):
    length = kw.shape[0]
    row, col = positions(length)
    causal = row >= col
    upto = causal.astype(F32).astype(BF16)
    table = decay_rows(dw[...], dn[...])
    col_wide, col_thin = columns(mm(upto, table, ((1,), (1,))))
    rows = mm(table, upto, ((1,), (1,)))
    row_wide = rows[0:1] + rows[1:2] + rows[2:3]
    row_thin = rows[3:4] + rows[4:5] + rows[5:6]

    def within(q, k, v, by_col, by_row):
        gap = jnp.where(causal, by_col - by_row, 0.0)
        fading = jnp.where(causal, jnp.exp(gap), 0.0)
        weights = mm(q[...], k[...], ((1,), (1,))) * k.shape[1] ** (-0.5) * fading
        return mm(weights.astype(BF16), v[...])

    at = vw.shape[1]
    out[:, :at] = within(qw, kw, vw, col_wide, row_wide)
    out[:, at:] = within(qn, kn, vn, col_thin, row_thin)


def unpack(x):
    x = x.astype(F32)
    cut = x.shape[-1] - LANES
    wide, thin = columns(x[:, cut:])
    return x[:, : cut - LANES], x[:, cut - LANES : cut], wide, thin


def after(earlier, latter):
    return (
        jnp.exp(latter[2]) * earlier[0] + latter[0],
        jnp.exp(latter[3]) * earlier[1] + latter[1],
        earlier[2] + latter[2],
        earlier[3] + latter[3],
    )


def put(ref, at, state, logs=True):
    rows, wide, thin = state[0].shape[0], state[0].shape[1], state[1].shape[1]
    ref[at, :, :wide] = state[0].astype(BF16)
    ref[at, :, wide : wide + thin] = state[1].astype(BF16)
    if logs:
        ref[at, :, wide + thin :] = log_lanes(state[2], state[3], rows).astype(BF16)


def of_chip(place, own, sibling, out):
    core, spot = place[0], place[1]
    first_core = core == 0
    pieces, rows = out.shape[0], out.shape[1]
    for d in range(pieces):
        start = pl.multiple_of(lax.rem(spot + d, pieces) * rows, rows)
        mine = own[core, pl.ds(start, rows), :]
        other = sibling[core, pl.ds(start, rows), :]
        first = jnp.where(first_core, mine, other)
        second = jnp.where(first_core, other, mine)
        put(out, d, after(unpack(first), unpack(second)))


def in_order(place, parts, ordered):
    pieces = len(parts)
    for d, part in enumerate(parts):
        ordered[lax.rem(place[1] - d + pieces, pieces)] = part[...]


def of_group(place, a, b, c, d, out, ordered):
    in_order(place, (a, b, c, d), ordered)
    total = unpack(ordered[0])
    for n in range(1, 4):
        total = after(total, unpack(ordered[n]))
    put(out, 0, total)


def before_each(place, a, b, c, d, near, mid, far, out, ordered, found):
    in_order(place, (a, b, c, d), ordered)
    state = after(after(unpack(far[0]), unpack(mid[0])), unpack(near[0]))
    for n in range(4):
        put(found, n, state, logs=False)
        state = after(state, unpack(ordered[n]))
    for n in range(4):
        out[n] = found[lax.rem(place[1] + n, 4)]


def gathered_half(place, a, b, c, d, out):
    parts = (a, b, c, d)
    rows = a.shape[0]
    for n, part in enumerate(parts):
        start = pl.multiple_of(lax.rem(place[1] - n + 4, 4) * rows, rows)
        out[pl.ds(start, rows), :] = part[...]


def heads_out(
    place, own_half, other_half, sibling, qw, qn, dw, dn, within, gw, gn, ow, on,
    far_a, far_b, right_a, right_b, left_a, left_b, own_a, own_b,
    came_wide, came_thin, turned_wide, turned_thin,
):
    first_core = place[0] == 0
    length = qw.shape[0]
    wide_width, thin_width = gw.shape[1], gn.shape[1]
    half_thin = came_thin.shape[0] // 2
    rows = own_half.shape[0]
    for h in range(2):
        mine = own_half[...] if h == 0 else other_half[...]
        other = other_half[...] if h == 0 else own_half[...]
        before = jnp.where(first_core, mine, other).astype(F32)
        s_wide, s_thin, l_wide, l_thin = unpack(sibling[h])
        b_wide, b_thin = before[:, :wide_width], before[:, wide_width:]
        wide = jnp.where(first_core, b_wide, jnp.exp(l_wide) * b_wide + s_wide)
        thin = jnp.where(first_core, b_thin, jnp.exp(l_thin) * b_thin + s_thin)
        came_wide[h * rows : (h + 1) * rows, :] = wide.astype(BF16)
        low = thin.astype(BF16)
        came_thin[h * half_thin : (h + 1) * half_thin, :LANES] = low[:half_thin]
        came_thin[h * half_thin : (h + 1) * half_thin, LANES:] = low[half_thin:]
    row, col = positions(length)
    upto = (row >= col).astype(F32).astype(BF16)
    cum_wide, cum_thin = columns(mm(upto, decay_rows(dw[...], dn[...]), ((1,), (1,))))

    def normed(q, came, cum, inner, gain):
        kept = inner + mm(q[...], came[...]) * jnp.exp(cum)
        centered = kept - jnp.mean(kept, axis=-1, keepdims=True)
        power = jnp.mean(centered * centered, axis=-1, keepdims=True)
        return (centered * lax.rsqrt(power + EPS) * gain[...]).astype(BF16)

    wide = normed(qw, came_wide, cum_wide, within[:, :wide_width], gw)
    thin = normed(qn, came_thin, cum_thin, within[:, wide_width:], gn)
    outs = (far_a, far_b, right_a, right_b, left_a, left_b, own_a, own_b)
    rows, members = far_a.shape[0], length // (2 * far_a.shape[0])
    for m in range(members):
        spot = lax.rem(m - place[2] + members, members)
        order = jnp.where(spot == 2, 0, jnp.where(spot == 1, 1, jnp.where(spot == 3, 2, 3)))
        start = pl.multiple_of(order * 2 * rows, 2 * rows)
        turned_wide[pl.ds(start, 2 * rows), :] = wide[m * 2 * rows : (m + 1) * 2 * rows]
        turned_thin[pl.ds(start, 2 * rows), :] = thin[m * 2 * rows : (m + 1) * 2 * rows]
    step = 512
    for n in range(ow.shape[1] // step):
        cols = slice(n * step, (n + 1) * step)
        done = (mm(turned_wide[...], ow[:, cols]) + mm(turned_thin[...], on[:, cols])).astype(BF16)
        for m, out in enumerate(outs):
            out[:, cols] = done[m * rows : (m + 1) * rows]


def add_two(a, b, c, d, first, second):
    first[...] = (a[...].astype(F32) + b[...].astype(F32)).astype(BF16)
    second[...] = (c[...].astype(F32) + d[...].astype(F32)).astype(BF16)


def rows_mid(
    own_a, left_a, right_a, own_b, left_b, right_b, stream, gain,
    mid_a, mid_b, normed_a, normed_b,
):
    rows = own_a.shape[0]
    halves = ((own_a, left_a, right_a, mid_a, normed_a), (own_b, left_b, right_b, mid_b, normed_b))
    for n, (own, left, right, middle, normed) in enumerate(halves):
        total = own[...].astype(F32) + left[...].astype(F32) + right[...].astype(F32)
        mid = (stream[n * rows : (n + 1) * rows].astype(F32) + total).astype(BF16)
        middle[...] = mid
        values = mid.astype(F32)
        power = jnp.mean(values * values, axis=-1, keepdims=True)
        normed[...] = (values * lax.rsqrt(power + EPS) * gain[...]).astype(BF16)


def hidden_rows(*refs):
    *ends, rows, up, down, total, hidden, done_rows, row_sems, up_sems, down_sems, out_sems = refs
    number = len(ends) // 2
    parts, weights, outs = ends[:number], ends[number], ends[number + 1 :]
    count, block, units = up.shape
    size = parts[0].shape[0]

    def fetch_rows(n, k):
        to = rows.at[k, pl.ds(n * size, size), :]
        return pltpu.make_async_copy(parts[n].at[:, pl.ds(k * block, block)], to, row_sems.at[n, k])

    def fetch(k, column, to, sems):
        start = pl.multiple_of(k * block, block)
        source = weights.at[pl.ds(start, block), pl.ds(column * units, units)]
        return pltpu.make_async_copy(source, to.at[k], sems.at[k])

    pairs = [(n, k) for k in range(count) for n in range(number)]
    for pair in pairs:
        fetch_rows(*pair).start()

    @pl.loop(0, count)
    def _(k):
        fetch(k, 0, up, up_sems).start()

    @pl.loop(0, count)
    def _(k):
        fetch(k, 1, down, down_sems).start()

    for pair in pairs:
        fetch_rows(*pair).wait()

    total[...] = jnp.zeros_like(total)

    @pl.loop(0, count)
    def _(k):
        fetch(k, 0, up, up_sems).wait()
        total[...] += mm(rows[k], up[k])

    raised = jnp.maximum(total[...], 0.0)
    hidden[...] = (raised * raised).astype(BF16)

    @pl.loop(0, count)
    def _(k):
        fetch(k, 1, down, down_sems).wait()
        start = pl.multiple_of(k * block, block)
        done = mm(hidden[...], down[k], ((1,), (1,))).astype(BF16)
        done_rows[:, pl.ds(start, block)] = done

    copies = []
    for n, out in enumerate(outs):
        source = done_rows.at[pl.ds(n * size, size), :]
        copies.append(pltpu.make_async_copy(source, out, out_sems.at[n]))
        copies[-1].start()
    for copy in copies:
        copy.wait()


def feed_forward(parts, weights):
    size, width = parts[0].shape
    units = weights.shape[1] // 2
    number, block = len(parts), 512
    count, total = width // block, number * size
    far = pl.BlockSpec(memory_space=pltpu.HBM)
    held = [pltpu.with_memory_space_constraint(p, pltpu.HBM) for p in (*parts, weights)]
    return pl.pallas_call(
        hidden_rows,
        out_shape=[pltpu.HBM((size, width), BF16)] * number,
        in_specs=[far] * (number + 1),
        out_specs=[far] * number,
        scratch_shapes=[
            pltpu.VMEM((count, total, block), BF16),
            pltpu.VMEM((count, block, units), BF16),
            pltpu.VMEM((count, block, units), BF16),
            pltpu.VMEM((total, units), F32),
            pltpu.VMEM((total, units), BF16),
            pltpu.VMEM((total, width), BF16),
            pltpu.SemaphoreType.DMA((number, count)),
            pltpu.SemaphoreType.DMA((count,)),
            pltpu.SemaphoreType.DMA((count,)),
            pltpu.SemaphoreType.DMA((number,)),
        ],
        compiler_params=pltpu.CompilerParams(vmem_limit_bytes=44 * 2**20),
        cost_estimate=pl.CostEstimate(
            flops=4 * total * width * units, bytes_accessed=4 * units * width, transcendentals=0
        ),
        name="hidden_rows",
    )(*held)


def last_sum(own_a, left_a, right_a, mid_a, own_b, left_b, right_b, mid_b, out):
    rows = own_a.shape[0]
    halves = ((own_a, left_a, right_a, mid_a), (own_b, left_b, right_b, mid_b))
    for n, parts in enumerate(halves):
        total = parts[3][...].astype(F32)
        for part in parts[:3]:
            total = total + part[...].astype(F32)
        out[n * rows : (n + 1) * rows] = total.astype(BF16)


def shift(x, axis, by, size, wrap=True):
    pairs = [(i, (i + by) % size) for i in range(size) if wrap or 0 <= i + by < size]
    return lax.ppermute(x, axis, pairs)


def swap(x):
    return lax.ppermute(x, "core", [(0, 1), (1, 0)])


def turn(x, by):
    return shift(x, "tp", by, lax.axis_size("tp"))


def reduced(far_a, far_b, right_a, right_b, left_a, left_b):
    came_far = turn(far_a, 1), turn(far_b, -1)
    came_right_b, came_left_a = turn(right_b, 1), turn(left_a, -1)
    like = [shaped(right_a.shape, BF16)] * 2
    right_sum, left_sum = call(
        add_two, like, Far(right_a), came_far[0], Far(left_b), came_far[1], far_out=True, limit=16
    )
    came = turn(right_sum, 1), came_right_b, came_left_a, turn(left_sum, -1)
    return came, right_sum


def spread(a, b):
    left_a, right_b = turn(a, 1), turn(b, -1)
    left_b, right_a = turn(b, 1), turn(a, -1)
    far_a, far_b = turn(left_a, 1), turn(right_b, -1)
    return far_a, far_b, right_a, right_b, left_a, left_b


def among(parts):
    return [parts[0]] + [shift(parts[d], "zb", d, 4) for d in range(1, 4)]


def on_device(
    stream_in, query_wide, key_wide, value_wide, query_narrow, key_narrow, value_narrow,
    decay_wide, decay_narrow, gain_wide, gain_narrow, out_wide, out_narrow, mlp_gain,
    up_weight, down_weight,
):
    members = lax.axis_size("tp")
    length, width = stream_in.shape
    portion = length // members
    member = lax.axis_index("tp")
    place = jnp.stack([lax.axis_index(n) for n in ("core", "zb", "tp")]).astype(jnp.int32)

    both = jnp.concatenate([up_weight, down_weight.T], axis=1)
    weights = lax.all_gather(both, SP, axis=0, tiled=True)

    wide_key, wide_value = key_wide.shape[1], value_wide.shape[1]
    thin_value = value_narrow.shape[1]
    half = wide_key // 2
    lanes = wide_value + 2 * LANES
    own = call(
        own_state, shaped((2, half, lanes), BF16),
        *map(Far, (key_wide, value_wide, decay_wide, key_narrow, value_narrow, decay_narrow)),
        flops=2 * length * wide_key * wide_value, moved=10**6,
    )
    sibling = swap(own)
    within = call(
        inside, shaped((length, wide_value + thin_value), F32),
        *map(Far, (query_wide, key_wide, value_wide, decay_wide)),
        *map(Far, (query_narrow, key_narrow, value_narrow, decay_narrow)),
        flops=6 * length * length * wide_value, moved=4 * 10**6,
    )
    rows = half // 4
    pieces = call(of_chip, shaped((4, rows, lanes), BF16), place, own, sibling)
    got = among([pieces[d] for d in range(4)])
    total = call(
        of_group, shaped((1, rows, lanes), BF16), place, *got,
        scratch=[pltpu.VMEM((4, rows, lanes), BF16)],
    )
    size = lax.axis_size("za")
    near, mid, far = [shift(total, "za", d, size, wrap=False) for d in range(1, 4)]
    found = call(
        before_each, shaped((4, rows, lanes - LANES), BF16), place, *got, near, mid, far,
        scratch=[pltpu.VMEM((4, rows, lanes), BF16), pltpu.VMEM((4, rows, lanes - LANES), BF16)],
    )
    back = among([found[d] for d in range(4)])
    own_half = call(gathered_half, shaped((half, lanes - LANES), BF16), place, *back)
    other_half = swap(own_half)
    quarter = portion // 2
    far_a, far_b, right_a, right_b, left_a, left_b, own_a, own_b = call(
        heads_out, [shaped((quarter, width), BF16)] * 8,
        place, own_half, other_half, sibling,
        *map(Far, (query_wide, query_narrow, decay_wide, decay_narrow)), within,
        *map(Far, (gain_wide[None], gain_narrow[None], out_wide, out_narrow)),
        scratch=[
            pltpu.VMEM((wide_key, wide_value), BF16),
            pltpu.VMEM((key_narrow.shape[1], thin_value), BF16),
            pltpu.VMEM((length, wide_value), BF16),
            pltpu.VMEM((length, thin_value), BF16),
        ],
        flops=4 * length * wide_value * width, moved=8 * 10**6, far_out=True,
    )
    came, _ = reduced(far_a, far_b, right_a, right_b, left_a, left_b)
    from_left_a, from_left_b, from_right_a, from_right_b = came
    own_stream = lax.dynamic_slice_in_dim(stream_in, member * portion, portion, 0)
    mid_a, mid_b, normed_a, normed_b = call(
        rows_mid, [shaped((quarter, width), BF16)] * 4,
        Far(own_a), from_left_a, from_right_a, Far(own_b), from_left_b, from_right_b,
        Far(own_stream), Far(mlp_gain[None]), far_out=True, limit=16,
    )
    others = feed_forward(spread(normed_a, normed_b), weights)
    came, sent = reduced(*others)
    from_left_a, from_left_b, from_right_a, from_right_b = came
    normed_a, normed_b, _ = lax.optimization_barrier((normed_a, normed_b, sent))
    own_a, own_b = feed_forward((normed_a, normed_b), weights)
    return call(
        last_sum, shaped((portion, width), BF16),
        Far(own_a), from_left_a, from_right_a, Far(mid_a),
        Far(own_b), from_left_b, from_right_b, Far(mid_b), far_out=True, limit=16,
    )


def solution(mesh):
    grp, sp, tp = mesh.shape["grp"], mesh.shape["sp"], mesh.shape["tp"]
    torus = Mesh(
        mesh.devices.reshape(grp, sp // 8, 4, 2, tp), ("grp", "za", "zb", "core", "tp")
    )
    placed = (
        P(GRP_SP, None),
        P(GRP_SP, "tp"),
        P(GRP_SP, "tp"),
        P(GRP_SP, "tp"),
        P(GRP_SP, "tp"),
        P(GRP_SP, "tp"),
        P(GRP_SP, "tp"),
        P("tp", GRP_SP),
        P("tp", GRP_SP),
        P("tp"),
        P("tp"),
        P("tp", None),
        P("tp", None),
        P(),
        P(SP, "tp"),
        P("tp", SP),
    )
    return jax.shard_map(
        on_device, mesh=torus, in_specs=placed, out_specs=P(GRP_SP_TP, None), check_vma=False
    )
```

```python
import jax
import jax.numpy as jnp
from jax import lax
from jax.experimental import pallas as pl
from jax.experimental.pallas import tpu as pltpu
from jax.sharding import Mesh
from jax.sharding import PartitionSpec as P

EPS = 1e-06
SP = ("za", "zb", "core")
GRP_SP = ("grp", "za", "zb", "core")
GRP_SP_TP = ("grp", "za", "zb", "core", "tp")
F32 = jnp.float32
BF16 = jnp.bfloat16
LANES = 128


def vmem():
    return pl.BlockSpec(memory_space=pltpu.VMEM)


def smem():
    return pl.BlockSpec(memory_space=pltpu.SMEM)


class Far:
    def __init__(self, x):
        self.x = x


def call(body, outs, *args, scratch=(), flops=0, moved=0, far_out=False, limit=48):
    many = isinstance(outs, (list, tuple))
    outs = list(outs) if many else [outs]
    pulled = [n for n, a in enumerate(args) if isinstance(a, Far)]
    args = [
        pltpu.with_memory_space_constraint(a.x, pltpu.HBM) if isinstance(a, Far) else a
        for a in args
    ]
    pushed = list(range(len(outs))) if far_out else []
    own = len(scratch)

    def inner(*refs):
        given, rest = list(refs[: len(args)]), list(refs[len(args) :])
        results, rest = rest[: len(outs)], rest[len(outs) :]
        kept, rest = rest[:own], rest[own:]
        held, sent = rest[: len(pulled)], rest[len(pulled) : len(pulled) + len(pushed)]
        sems = rest[-1]
        copies = []
        for k, n in enumerate(pulled):
            copies.append(pltpu.make_async_copy(given[n], held[k], sems.at[k]))
            copies[-1].start()
            given[n] = held[k]
        for copy in copies:
            copy.wait()
        body(*given, *(sent if pushed else results), *kept)
        copies = []
        for k in range(len(pushed)):
            copies.append(pltpu.make_async_copy(sent[k], results[k], sems.at[len(pulled) + k]))
            copies[-1].start()
        for copy in copies:
            copy.wait()

    far = pl.BlockSpec(memory_space=pltpu.HBM)
    specs = [
        smem() if a.dtype == jnp.int32 else far if n in pulled else vmem()
        for n, a in enumerate(args)
    ]
    buffers = [pltpu.VMEM(args[n].shape, args[n].dtype) for n in pulled]
    buffers += [pltpu.VMEM(outs[n].shape, outs[n].dtype) for n in pushed]
    result = pl.pallas_call(
        inner,
        out_shape=[pltpu.HBM(o.shape, o.dtype) for o in outs] if far_out else outs,
        in_specs=specs,
        out_specs=[far if far_out else vmem() for _ in outs],
        scratch_shapes=[
            *scratch, *buffers, pltpu.SemaphoreType.DMA((max(len(pulled) + len(pushed), 1),))
        ],
        compiler_params=pltpu.CompilerParams(vmem_limit_bytes=limit * 2**20),
        cost_estimate=pl.CostEstimate(flops=flops, bytes_accessed=moved, transcendentals=0),
        name=body.__name__,
    )(*args)
    return result if many else result[0]


def shaped(shape, dtype):
    return jax.ShapeDtypeStruct(shape, dtype)


def mm(a, b, dims=((1,), (0,))):
    return lax.dot_general(a, b, (dims, ((), ())), preferred_element_type=F32)


def three(x):
    high = x.astype(BF16).astype(F32)
    mid = (x - high).astype(BF16).astype(F32)
    low = (x - high - mid).astype(BF16).astype(F32)
    return high, mid, low


def pick(index, values):
    out = jnp.zeros_like(index, dtype=F32)
    for n, value in enumerate(values):
        out = jnp.where(index == n, value, out)
    return out


def decay_rows(dw, dn):
    row = lax.broadcasted_iota(jnp.int32, (8, dw.shape[1]), 0)
    return pick(row, three(dw) + three(dn)).astype(BF16)


def columns(table):
    wide = table[:, 0:1] + table[:, 1:2] + table[:, 2:3]
    thin = table[:, 3:4] + table[:, 4:5] + table[:, 5:6]
    return wide, thin


def log_lanes(wide, thin, rows):
    lane = lax.broadcasted_iota(jnp.int32, (rows, LANES), 1)
    return pick(lane, three(wide) + three(thin))


def positions(length):
    row = lax.broadcasted_iota(jnp.int32, (length, length), 0)
    col = lax.broadcasted_iota(jnp.int32, (length, length), 1)
    return row, col


def own_state(kw, vw, dw, kn, vn, dn, out):
    length = kw.shape[0]
    row, col = positions(length)
    later = (col > row).astype(F32).astype(BF16)
    table = decay_rows(dw[...], dn[...])
    end_wide, end_thin = columns(mm(later, table, ((1,), (1,))))
    total_wide = jnp.sum(dw[...], axis=1, keepdims=True)
    total_thin = jnp.sum(dn[...], axis=1, keepdims=True)

    def state(k, v, end):
        keyed = k[...].astype(F32) * k.shape[1] ** (-0.5) * jnp.exp(end)
        return mm(keyed.astype(BF16), v[...], ((0,), (0,))).astype(BF16)

    wide = state(kw, vw, end_wide)
    thin = state(kn, vn, end_thin)
    half_wide, half_thin = wide.shape[0] // 2, thin.shape[0] // 2
    at = wide.shape[1]
    logs = log_lanes(total_wide, total_thin, half_wide).astype(BF16)
    for h in range(2):
        out[h, :, :at] = wide[h * half_wide : (h + 1) * half_wide]
        part = thin[h * half_thin : (h + 1) * half_thin]
        out[h, :half_thin, at : at + LANES] = part[:, :LANES]
        out[h, half_thin:, at : at + LANES] = part[:, LANES:]
        out[h, :, at + LANES :] = logs


def inside(qw, kw, vw, dw, qn, kn, vn, dn, out):
    length = kw.shape[0]
    row, col = positions(length)
    causal = row >= col
    upto = causal.astype(F32).astype(BF16)
    table = decay_rows(dw[...], dn[...])
    col_wide, col_thin = columns(mm(upto, table, ((1,), (1,))))
    rows = mm(table, upto, ((1,), (1,)))
    row_wide = rows[0:1] + rows[1:2] + rows[2:3]
    row_thin = rows[3:4] + rows[4:5] + rows[5:6]

    def within(q, k, v, by_col, by_row):
        gap = jnp.where(causal, by_col - by_row, 0.0)
        fading = jnp.where(causal, jnp.exp(gap), 0.0)
        weights = mm(q[...], k[...], ((1,), (1,))) * k.shape[1] ** (-0.5) * fading
        return mm(weights.astype(BF16), v[...])

    at = vw.shape[1]
    out[:, :at] = within(qw, kw, vw, col_wide, row_wide)
    out[:, at:] = within(qn, kn, vn, col_thin, row_thin)


def unpack(x):
    x = x.astype(F32)
    cut = x.shape[-1] - LANES
    wide, thin = columns(x[:, cut:])
    return x[:, : cut - LANES], x[:, cut - LANES : cut], wide, thin


def after(earlier, latter):
    return (
        jnp.exp(latter[2]) * earlier[0] + latter[0],
        jnp.exp(latter[3]) * earlier[1] + latter[1],
        earlier[2] + latter[2],
        earlier[3] + latter[3],
    )


def put(ref, at, state, logs=True):
    rows, wide, thin = state[0].shape[0], state[0].shape[1], state[1].shape[1]
    ref[at, :, :wide] = state[0].astype(BF16)
    ref[at, :, wide : wide + thin] = state[1].astype(BF16)
    if logs:
        ref[at, :, wide + thin :] = log_lanes(state[2], state[3], rows).astype(BF16)


def of_chip(place, own, sibling, out):
    core, spot = place[0], place[1]
    first_core = core == 0
    pieces, rows = out.shape[0], out.shape[1]
    for d in range(pieces):
        start = pl.multiple_of(lax.rem(spot + d, pieces) * rows, rows)
        mine = own[core, pl.ds(start, rows), :]
        other = sibling[core, pl.ds(start, rows), :]
        first = jnp.where(first_core, mine, other)
        second = jnp.where(first_core, other, mine)
        put(out, d, after(unpack(first), unpack(second)))


def in_order(place, parts, ordered):
    pieces = len(parts)
    for d, part in enumerate(parts):
        ordered[lax.rem(place[1] - d + pieces, pieces)] = part[...]


def of_group(place, a, b, c, d, out, ordered):
    in_order(place, (a, b, c, d), ordered)
    total = unpack(ordered[0])
    for n in range(1, 4):
        total = after(total, unpack(ordered[n]))
    put(out, 0, total)


def before_each(place, a, b, c, d, near, mid, far, out, ordered, found):
    in_order(place, (a, b, c, d), ordered)
    state = after(after(unpack(far[0]), unpack(mid[0])), unpack(near[0]))
    for n in range(4):
        put(found, n, state, logs=False)
        state = after(state, unpack(ordered[n]))
    for n in range(4):
        out[n] = found[lax.rem(place[1] + n, 4)]


def gathered_half(place, a, b, c, d, out):
    parts = (a, b, c, d)
    rows = a.shape[0]
    for n, part in enumerate(parts):
        start = pl.multiple_of(lax.rem(place[1] - n + 4, 4) * rows, rows)
        out[pl.ds(start, rows), :] = part[...]


def heads_out(
    place, own_half, other_half, sibling, qw, qn, dw, dn, within, gw, gn, ow, on,
    far_a, far_b, right_a, right_b, left_a, left_b, own_a, own_b,
    came_wide, came_thin, turned_wide, turned_thin,
):
    first_core = place[0] == 0
    length = qw.shape[0]
    wide_width, thin_width = gw.shape[1], gn.shape[1]
    half_thin = came_thin.shape[0] // 2
    rows = own_half.shape[0]
    for h in range(2):
        mine = own_half[...] if h == 0 else other_half[...]
        other = other_half[...] if h == 0 else own_half[...]
        before = jnp.where(first_core, mine, other).astype(F32)
        s_wide, s_thin, l_wide, l_thin = unpack(sibling[h])
        b_wide, b_thin = before[:, :wide_width], before[:, wide_width:]
        wide = jnp.where(first_core, b_wide, jnp.exp(l_wide) * b_wide + s_wide)
        thin = jnp.where(first_core, b_thin, jnp.exp(l_thin) * b_thin + s_thin)
        came_wide[h * rows : (h + 1) * rows, :] = wide.astype(BF16)
        low = thin.astype(BF16)
        came_thin[h * half_thin : (h + 1) * half_thin, :LANES] = low[:half_thin]
        came_thin[h * half_thin : (h + 1) * half_thin, LANES:] = low[half_thin:]
    row, col = positions(length)
    upto = (row >= col).astype(F32).astype(BF16)
    cum_wide, cum_thin = columns(mm(upto, decay_rows(dw[...], dn[...]), ((1,), (1,))))

    def normed(q, came, cum, inner, gain):
        kept = inner + mm(q[...], came[...]) * jnp.exp(cum)
        centered = kept - jnp.mean(kept, axis=-1, keepdims=True)
        power = jnp.mean(centered * centered, axis=-1, keepdims=True)
        return (centered * lax.rsqrt(power + EPS) * gain[...]).astype(BF16)

    wide = normed(qw, came_wide, cum_wide, within[:, :wide_width], gw)
    thin = normed(qn, came_thin, cum_thin, within[:, wide_width:], gn)
    outs = (far_a, far_b, right_a, right_b, left_a, left_b, own_a, own_b)
    rows, members = far_a.shape[0], length // (2 * far_a.shape[0])
    for m in range(members):
        spot = lax.rem(m - place[2] + members, members)
        order = jnp.where(spot == 2, 0, jnp.where(spot == 1, 1, jnp.where(spot == 3, 2, 3)))
        start = pl.multiple_of(order * 2 * rows, 2 * rows)
        turned_wide[pl.ds(start, 2 * rows), :] = wide[m * 2 * rows : (m + 1) * 2 * rows]
        turned_thin[pl.ds(start, 2 * rows), :] = thin[m * 2 * rows : (m + 1) * 2 * rows]
    step = 1024

    @pl.loop(0, ow.shape[1] // step)
    def _(n):
        cols = pl.ds(pl.multiple_of(n * step, step), step)
        done = (mm(turned_wide[...], ow[:, cols]) + mm(turned_thin[...], on[:, cols])).astype(BF16)
        for m, out in enumerate(outs):
            out[:, cols] = done[m * rows : (m + 1) * rows]


def add_two(a, b, c, d, first, second):
    first[...] = (a[...].astype(F32) + b[...].astype(F32)).astype(BF16)
    second[...] = (c[...].astype(F32) + d[...].astype(F32)).astype(BF16)


def rows_mid(
    own_a, left_a, right_a, own_b, left_b, right_b, stream, gain,
    mid_a, mid_b, normed_a, normed_b,
):
    rows = own_a.shape[0]
    halves = ((own_a, left_a, right_a, mid_a, normed_a), (own_b, left_b, right_b, mid_b, normed_b))
    for n, (own, left, right, middle, normed) in enumerate(halves):
        total = own[...].astype(F32) + left[...].astype(F32) + right[...].astype(F32)
        mid = (stream[n * rows : (n + 1) * rows].astype(F32) + total).astype(BF16)
        middle[...] = mid
        values = mid.astype(F32)
        power = jnp.mean(values * values, axis=-1, keepdims=True)
        normed[...] = (values * lax.rsqrt(power + EPS) * gain[...]).astype(BF16)


def fetched(pairs, sems):
    copies = [pltpu.make_async_copy(a, b, sems.at[n]) for n, (a, b) in enumerate(pairs)]
    for copy in copies:
        copy.start()
    return copies


def stacked(parts, rows):
    size = parts[0].shape[0]
    return [rows.at[pl.ds(n * size, size), :] for n in range(len(parts))]


def squared(x):
    raised = jnp.maximum(x, 0.0)
    return (raised * raised).astype(BF16)


def first_rows(
    a, b, weights, out_a, out_b, up, down, rows, total, hidden, row_sems, up_sems, down_sems
):
    units, block = up.shape[1], 512
    count = up.shape[0] // block

    def fetch(k, column, to, sems):
        span = pl.ds(pl.multiple_of(k * block, block), block)
        source = weights.at[span, pl.ds(column * units, units)]
        return pltpu.make_async_copy(source, to.at[span, :], sems.at[k])

    copies = fetched(list(zip((a, b), stacked((a, b), rows))), row_sems)

    @pl.loop(0, count)
    def _(k):
        fetch(k, 0, up, up_sems).start()

    @pl.loop(0, count)
    def _(k):
        fetch(k, 1, down, down_sems).start()

    for copy in copies:
        copy.wait()
    total[...] = jnp.zeros_like(total)

    @pl.loop(0, count)
    def _(k):
        fetch(k, 0, up, up_sems).wait()
        span = pl.ds(pl.multiple_of(k * block, block), block)
        total[...] += mm(rows[:, span], up[span, :])

    hidden[...] = squared(total[...])

    @pl.loop(0, count)
    def _(k):
        fetch(k, 1, down, down_sems).wait()
        span = pl.ds(pl.multiple_of(k * block, block), block)
        rows[:, span] = mm(hidden[...], down[span, :], ((1,), (1,))).astype(BF16)

    for copy in fetched(list(zip(stacked((a, b), rows), (out_a, out_b))), row_sems):
        copy.wait()


def more_rows(*refs):
    *ends, rows, hidden, row_sems = refs
    number = (len(ends) - 2) // 2
    parts, (up, down), outs = ends[:number], ends[number : number + 2], ends[number + 2 :]
    size, block = parts[0].shape[0], 1024
    for copy in fetched(list(zip(parts, stacked(parts, rows))), row_sems):
        copy.wait()

    @pl.loop(0, up.shape[1] // block)
    def _(n):
        cols = pl.ds(pl.multiple_of(n * block, block), block)
        hidden[:, cols] = squared(mm(rows[...], up[:, cols]))

    @pl.loop(0, down.shape[0] // block)
    def _(n):
        cols = pl.ds(pl.multiple_of(n * block, block), block)
        done = mm(hidden[...], down[cols, :], ((1,), (1,))).astype(BF16)
        for m, out in enumerate(outs):
            out[:, cols] = done[m * size : (m + 1) * size]


def first_forward(parts, weights):
    size, width = parts[0].shape
    units = weights.shape[1] // 2
    count, total = width // 512, 2 * size
    far = pl.BlockSpec(memory_space=pltpu.HBM)
    held = [pltpu.with_memory_space_constraint(p, pltpu.HBM) for p in (*parts, weights)]
    out_a, out_b, up, down = pl.pallas_call(
        first_rows,
        out_shape=[pltpu.HBM((size, width), BF16)] * 2 + [pltpu.VMEM((width, units), BF16)] * 2,
        in_specs=[far] * 3,
        out_specs=[far] * 2 + [vmem()] * 2,
        scratch_shapes=[
            pltpu.VMEM((total, width), BF16),
            pltpu.VMEM((total, units), F32),
            pltpu.VMEM((total, units), BF16),
            pltpu.SemaphoreType.DMA((2,)),
            pltpu.SemaphoreType.DMA((count,)),
            pltpu.SemaphoreType.DMA((count,)),
        ],
        compiler_params=pltpu.CompilerParams(vmem_limit_bytes=16 * 2**20),
        cost_estimate=pl.CostEstimate(
            flops=4 * total * width * units, bytes_accessed=4 * units * width, transcendentals=0
        ),
        name="first_rows",
    )(*held)
    return out_a, out_b, (up, down)


def more_forward(parts, weights):
    size, width = parts[0].shape
    units = weights[0].shape[1]
    number = len(parts)
    total = number * size
    far = pl.BlockSpec(memory_space=pltpu.HBM)
    held = list(parts)
    held += [pltpu.with_memory_space_constraint(w, pltpu.VMEM) for w in weights]
    return pl.pallas_call(
        more_rows,
        out_shape=[shaped((size, width), BF16)] * number,
        in_specs=[pl.BlockSpec(memory_space=pl.ANY)] * number + [vmem()] * 2,
        out_specs=[vmem()] * number,
        scratch_shapes=[
            pltpu.VMEM((total, width), BF16),
            pltpu.VMEM((total, units), BF16),
            pltpu.SemaphoreType.DMA((number,)),
        ],
        compiler_params=pltpu.CompilerParams(vmem_limit_bytes=24 * 2**20),
        cost_estimate=pl.CostEstimate(
            flops=4 * total * width * units, bytes_accessed=4 * units * width, transcendentals=0
        ),
        name="more_rows",
    )(*held)


def last_sum(own_a, left_a, right_a, mid_a, own_b, left_b, right_b, mid_b, out):
    rows = own_a.shape[0]
    halves = ((own_a, left_a, right_a, mid_a), (own_b, left_b, right_b, mid_b))
    for n, parts in enumerate(halves):
        total = parts[3][...].astype(F32)
        for part in parts[:3]:
            total = total + part[...].astype(F32)
        out[n * rows : (n + 1) * rows] = total.astype(BF16)


def shift(x, axis, by, size, wrap=True):
    pairs = [(i, (i + by) % size) for i in range(size) if wrap or 0 <= i + by < size]
    return lax.ppermute(x, axis, pairs)


def swap(x):
    return lax.ppermute(x, "core", [(0, 1), (1, 0)])


def turn(x, by):
    return shift(x, "tp", by, lax.axis_size("tp"))


def sent_far(far_a, far_b):
    return turn(far_a, 1), turn(far_b, -1)


def reduced(came_far, right_a, right_b, left_a, left_b, near=False):
    came_right_b, came_left_a = turn(right_b, 1), turn(left_a, -1)
    like = [shaped(right_a.shape, BF16)] * 2
    held = (right_a, left_b) if near else (Far(right_a), Far(left_b))
    right_sum, left_sum = call(
        add_two, like, held[0], came_far[0], held[1], came_far[1], far_out=not near, limit=16
    )
    came = turn(right_sum, 1), came_right_b, came_left_a, turn(left_sum, -1)
    return came, right_sum


def spread(a, b):
    left_a, right_b = turn(a, 1), turn(b, -1)
    left_b, right_a = turn(b, 1), turn(a, -1)
    far_a, far_b = turn(left_a, 1), turn(right_b, -1)
    return far_a, far_b, right_a, right_b, left_a, left_b


def among(parts):
    return [parts[0]] + [shift(parts[d], "zb", d, 4) for d in range(1, 4)]


def on_device(
    stream_in, query_wide, key_wide, value_wide, query_narrow, key_narrow, value_narrow,
    decay_wide, decay_narrow, gain_wide, gain_narrow, out_wide, out_narrow, mlp_gain,
    up_weight, down_weight,
):
    members = lax.axis_size("tp")
    length, width = stream_in.shape
    portion = length // members
    member = lax.axis_index("tp")
    place = jnp.stack([lax.axis_index(n) for n in ("core", "zb", "tp")]).astype(jnp.int32)

    both = jnp.concatenate([up_weight, down_weight.T], axis=1)
    weights = lax.all_gather(both, SP, axis=0, tiled=True)

    wide_key, wide_value = key_wide.shape[1], value_wide.shape[1]
    thin_value = value_narrow.shape[1]
    half = wide_key // 2
    lanes = wide_value + 2 * LANES
    own = call(
        own_state, shaped((2, half, lanes), BF16),
        *map(Far, (key_wide, value_wide, decay_wide, key_narrow, value_narrow, decay_narrow)),
        flops=2 * length * wide_key * wide_value, moved=10**6,
    )
    sibling = swap(own)
    within = call(
        inside, shaped((length, wide_value + thin_value), F32),
        *map(Far, (query_wide, key_wide, value_wide, decay_wide)),
        *map(Far, (query_narrow, key_narrow, value_narrow, decay_narrow)),
        flops=6 * length * length * wide_value, moved=4 * 10**6,
    )
    rows = half // 4
    pieces = call(of_chip, shaped((4, rows, lanes), BF16), place, own, sibling)
    got = among([pieces[d] for d in range(4)])
    total = call(
        of_group, shaped((1, rows, lanes), BF16), place, *got,
        scratch=[pltpu.VMEM((4, rows, lanes), BF16)],
    )
    size = lax.axis_size("za")
    near, far = [shift(total, "za", d, size, wrap=False) for d in (1, 3)]
    mid = shift(near, "za", 1, size, wrap=False)
    found = call(
        before_each, shaped((4, rows, lanes - LANES), BF16), place, *got, near, mid, far,
        scratch=[pltpu.VMEM((4, rows, lanes), BF16), pltpu.VMEM((4, rows, lanes - LANES), BF16)],
    )
    back = among([found[d] for d in range(4)])
    own_half = call(gathered_half, shaped((half, lanes - LANES), BF16), place, *back)
    other_half = swap(own_half)
    quarter = portion // 2
    far_a, far_b, right_a, right_b, left_a, left_b, own_a, own_b = call(
        heads_out, [shaped((quarter, width), BF16)] * 8,
        place, own_half, other_half, sibling,
        *map(Far, (query_wide, query_narrow, decay_wide, decay_narrow)), within,
        *map(Far, (gain_wide[None], gain_narrow[None], out_wide, out_narrow)),
        scratch=[
            pltpu.VMEM((wide_key, wide_value), BF16),
            pltpu.VMEM((key_narrow.shape[1], thin_value), BF16),
            pltpu.VMEM((length, wide_value), BF16),
            pltpu.VMEM((length, thin_value), BF16),
        ],
        flops=4 * length * wide_value * width, moved=8 * 10**6, far_out=True,
    )
    came, _ = reduced(sent_far(far_a, far_b), right_a, right_b, left_a, left_b)
    from_left_a, from_left_b, from_right_a, from_right_b = came
    own_stream = lax.dynamic_slice_in_dim(stream_in, member * portion, portion, 0)
    mid_a, mid_b, normed_a, normed_b = call(
        rows_mid, [shaped((quarter, width), BF16)] * 4,
        Far(own_a), from_left_a, from_right_a, Far(own_b), from_left_b, from_right_b,
        Far(own_stream), Far(mlp_gain[None]), far_out=True, limit=16,
    )
    far_a, far_b, *others = spread(normed_a, normed_b)
    far_a, far_b, kept = first_forward((far_a, far_b), weights)
    came_far = sent_far(far_a, far_b)
    came, sent = reduced(came_far, *more_forward(others, kept), near=True)
    from_left_a, from_left_b, from_right_a, from_right_b = came
    normed_a, normed_b, _ = lax.optimization_barrier((normed_a, normed_b, sent))
    own_a, own_b = more_forward((normed_a, normed_b), kept)
    return call(
        last_sum, shaped((portion, width), BF16),
        own_a, from_left_a, from_right_a, Far(mid_a),
        own_b, from_left_b, from_right_b, Far(mid_b), far_out=True, limit=16,
    )


def solution(mesh):
    grp, sp, tp = mesh.shape["grp"], mesh.shape["sp"], mesh.shape["tp"]
    torus = Mesh(
        mesh.devices.reshape(grp, sp // 8, 4, 2, tp), ("grp", "za", "zb", "core", "tp")
    )
    placed = (
        P(GRP_SP, None),
        P(GRP_SP, "tp"),
        P(GRP_SP, "tp"),
        P(GRP_SP, "tp"),
        P(GRP_SP, "tp"),
        P(GRP_SP, "tp"),
        P(GRP_SP, "tp"),
        P("tp", GRP_SP),
        P("tp", GRP_SP),
        P("tp"),
        P("tp"),
        P("tp", None),
        P("tp", None),
        P(),
        P(SP, "tp"),
        P("tp", SP),
    )
    return jax.shard_map(
        on_device, mesh=torus, in_specs=placed, out_specs=P(GRP_SP_TP, None), check_vma=False
    )
```

```python
import jax
import jax.numpy as jnp
from jax import lax
from jax.experimental import pallas as pl
from jax.experimental.pallas import tpu as pltpu
from jax.sharding import Mesh
from jax.sharding import PartitionSpec as P

EPS = 1e-06
SP = ("za", "zb", "core")
GRP_SP = ("grp", "za", "zb", "core")
GRP_SP_TP = ("grp", "za", "zb", "core", "tp")
F32 = jnp.float32
BF16 = jnp.bfloat16
LANES = 128


def vmem():
    return pl.BlockSpec(memory_space=pltpu.VMEM)


def smem():
    return pl.BlockSpec(memory_space=pltpu.SMEM)


class Far:
    def __init__(self, x):
        self.x = x


def call(body, outs, *args, scratch=(), flops=0, moved=0, far_out=False, limit=48):
    many = isinstance(outs, (list, tuple))
    outs = list(outs) if many else [outs]
    pulled = [n for n, a in enumerate(args) if isinstance(a, Far)]
    args = [
        pltpu.with_memory_space_constraint(a.x, pltpu.HBM) if isinstance(a, Far) else a
        for a in args
    ]
    pushed = list(range(len(outs))) if far_out else []
    own = len(scratch)

    def inner(*refs):
        given, rest = list(refs[: len(args)]), list(refs[len(args) :])
        results, rest = rest[: len(outs)], rest[len(outs) :]
        kept, rest = rest[:own], rest[own:]
        held, sent = rest[: len(pulled)], rest[len(pulled) : len(pulled) + len(pushed)]
        sems = rest[-1]
        copies = []
        for k, n in enumerate(pulled):
            copies.append(pltpu.make_async_copy(given[n], held[k], sems.at[k]))
            copies[-1].start()
            given[n] = held[k]
        for copy in copies:
            copy.wait()
        body(*given, *(sent if pushed else results), *kept)
        copies = []
        for k in range(len(pushed)):
            copies.append(pltpu.make_async_copy(sent[k], results[k], sems.at[len(pulled) + k]))
            copies[-1].start()
        for copy in copies:
            copy.wait()

    far = pl.BlockSpec(memory_space=pltpu.HBM)
    specs = [
        smem() if a.dtype == jnp.int32 else far if n in pulled else vmem()
        for n, a in enumerate(args)
    ]
    buffers = [pltpu.VMEM(args[n].shape, args[n].dtype) for n in pulled]
    buffers += [pltpu.VMEM(outs[n].shape, outs[n].dtype) for n in pushed]
    result = pl.pallas_call(
        inner,
        out_shape=[pltpu.HBM(o.shape, o.dtype) for o in outs] if far_out else outs,
        in_specs=specs,
        out_specs=[far if far_out else vmem() for _ in outs],
        scratch_shapes=[
            *scratch, *buffers, pltpu.SemaphoreType.DMA((max(len(pulled) + len(pushed), 1),))
        ],
        compiler_params=pltpu.CompilerParams(vmem_limit_bytes=limit * 2**20),
        cost_estimate=pl.CostEstimate(flops=flops, bytes_accessed=moved, transcendentals=0),
        name=body.__name__,
    )(*args)
    return result if many else result[0]


def shaped(shape, dtype):
    return jax.ShapeDtypeStruct(shape, dtype)


def mm(a, b, dims=((1,), (0,))):
    return lax.dot_general(a, b, (dims, ((), ())), preferred_element_type=F32)


def three(x):
    high = x.astype(BF16).astype(F32)
    mid = (x - high).astype(BF16).astype(F32)
    low = (x - high - mid).astype(BF16).astype(F32)
    return high, mid, low


def pick(index, values):
    out = jnp.zeros_like(index, dtype=F32)
    for n, value in enumerate(values):
        out = jnp.where(index == n, value, out)
    return out


def decay_rows(dw, dn):
    row = lax.broadcasted_iota(jnp.int32, (8, dw.shape[1]), 0)
    return pick(row, three(dw) + three(dn)).astype(BF16)


def columns(table):
    wide = table[:, 0:1] + table[:, 1:2] + table[:, 2:3]
    thin = table[:, 3:4] + table[:, 4:5] + table[:, 5:6]
    return wide, thin


def log_lanes(wide, thin, rows):
    lane = lax.broadcasted_iota(jnp.int32, (rows, LANES), 1)
    return pick(lane, three(wide) + three(thin))


def positions(length):
    row = lax.broadcasted_iota(jnp.int32, (length, length), 0)
    col = lax.broadcasted_iota(jnp.int32, (length, length), 1)
    return row, col


def own_state(kw, vw, dw, kn, vn, dn, out):
    length = kw.shape[0]
    row, col = positions(length)
    later = (col > row).astype(F32).astype(BF16)
    table = decay_rows(dw[...], dn[...])
    end_wide, end_thin = columns(mm(later, table, ((1,), (1,))))
    total_wide = jnp.sum(dw[...], axis=1, keepdims=True)
    total_thin = jnp.sum(dn[...], axis=1, keepdims=True)

    def state(k, v, end):
        keyed = k[...].astype(F32) * k.shape[1] ** (-0.5) * jnp.exp(end)
        return mm(keyed.astype(BF16), v[...], ((0,), (0,))).astype(BF16)

    wide = state(kw, vw, end_wide)
    thin = state(kn, vn, end_thin)
    half_wide, half_thin = wide.shape[0] // 2, thin.shape[0] // 2
    at = wide.shape[1]
    logs = log_lanes(total_wide, total_thin, half_wide).astype(BF16)
    for h in range(2):
        out[h, :, :at] = wide[h * half_wide : (h + 1) * half_wide]
        part = thin[h * half_thin : (h + 1) * half_thin]
        out[h, :half_thin, at : at + LANES] = part[:, :LANES]
        out[h, half_thin:, at : at + LANES] = part[:, LANES:]
        out[h, :, at + LANES :] = logs


def inside(qw, kw, vw, dw, qn, kn, vn, dn, out):
    length = kw.shape[0]
    row, col = positions(length)
    causal = row >= col
    upto = causal.astype(F32).astype(BF16)
    table = decay_rows(dw[...], dn[...])
    col_wide, col_thin = columns(mm(upto, table, ((1,), (1,))))
    rows = mm(table, upto, ((1,), (1,)))
    row_wide = rows[0:1] + rows[1:2] + rows[2:3]
    row_thin = rows[3:4] + rows[4:5] + rows[5:6]

    def within(q, k, v, by_col, by_row):
        gap = jnp.where(causal, by_col - by_row, 0.0)
        fading = jnp.where(causal, jnp.exp(gap), 0.0)
        weights = mm(q[...], k[...], ((1,), (1,))) * k.shape[1] ** (-0.5) * fading
        return mm(weights.astype(BF16), v[...])

    at = vw.shape[1]
    out[:, :at] = within(qw, kw, vw, col_wide, row_wide)
    out[:, at:] = within(qn, kn, vn, col_thin, row_thin)


def unpack(x):
    x = x.astype(F32)
    cut = x.shape[-1] - LANES
    wide, thin = columns(x[:, cut:])
    return x[:, : cut - LANES], x[:, cut - LANES : cut], wide, thin


def after(earlier, latter):
    return (
        jnp.exp(latter[2]) * earlier[0] + latter[0],
        jnp.exp(latter[3]) * earlier[1] + latter[1],
        earlier[2] + latter[2],
        earlier[3] + latter[3],
    )


def put(ref, at, state, logs=True):
    rows, wide, thin = state[0].shape[0], state[0].shape[1], state[1].shape[1]
    ref[at, :, :wide] = state[0].astype(BF16)
    ref[at, :, wide : wide + thin] = state[1].astype(BF16)
    if logs:
        ref[at, :, wide + thin :] = log_lanes(state[2], state[3], rows).astype(BF16)


def of_chip(place, own, sibling, out):
    core, spot = place[0], place[1]
    first_core = core == 0
    pieces, rows = out.shape[0], out.shape[1]
    for d in range(pieces):
        start = pl.multiple_of(lax.rem(spot + d, pieces) * rows, rows)
        mine = own[core, pl.ds(start, rows), :]
        other = sibling[core, pl.ds(start, rows), :]
        first = jnp.where(first_core, mine, other)
        second = jnp.where(first_core, other, mine)
        put(out, d, after(unpack(first), unpack(second)))


def in_order(place, parts, ordered):
    pieces = len(parts)
    for d, part in enumerate(parts):
        ordered[lax.rem(place[1] - d + pieces, pieces)] = part[...]


def of_group(place, a, b, c, d, out, ordered):
    in_order(place, (a, b, c, d), ordered)
    total = unpack(ordered[0])
    for n in range(1, 4):
        total = after(total, unpack(ordered[n]))
    put(out, 0, total)


def before_each(place, a, b, c, d, near, mid, far, out, ordered, found):
    in_order(place, (a, b, c, d), ordered)
    state = after(after(unpack(far[0]), unpack(mid[0])), unpack(near[0]))
    for n in range(4):
        put(found, n, state, logs=False)
        state = after(state, unpack(ordered[n]))
    for n in range(4):
        out[n] = found[lax.rem(place[1] + n, 4)]


def gathered_half(place, a, b, c, d, out):
    parts = (a, b, c, d)
    rows = a.shape[0]
    for n, part in enumerate(parts):
        start = pl.multiple_of(lax.rem(place[1] - n + 4, 4) * rows, rows)
        out[pl.ds(start, rows), :] = part[...]


def heads_out(
    place, own_half, other_half, sibling, qw, qn, dw, dn, within, gw, gn, ow, on,
    far_a, far_b, right_a, right_b, left_a, left_b, own_a, own_b,
    came_wide, came_thin, turned_wide, turned_thin,
):
    first_core = place[0] == 0
    length = qw.shape[0]
    wide_width, thin_width = gw.shape[1], gn.shape[1]
    half_thin = came_thin.shape[0] // 2
    rows = own_half.shape[0]
    for h in range(2):
        mine = own_half[...] if h == 0 else other_half[...]
        other = other_half[...] if h == 0 else own_half[...]
        before = jnp.where(first_core, mine, other).astype(F32)
        s_wide, s_thin, l_wide, l_thin = unpack(sibling[h])
        b_wide, b_thin = before[:, :wide_width], before[:, wide_width:]
        wide = jnp.where(first_core, b_wide, jnp.exp(l_wide) * b_wide + s_wide)
        thin = jnp.where(first_core, b_thin, jnp.exp(l_thin) * b_thin + s_thin)
        came_wide[h * rows : (h + 1) * rows, :] = wide.astype(BF16)
        low = thin.astype(BF16)
        came_thin[h * half_thin : (h + 1) * half_thin, :LANES] = low[:half_thin]
        came_thin[h * half_thin : (h + 1) * half_thin, LANES:] = low[half_thin:]
    row, col = positions(length)
    upto = (row >= col).astype(F32).astype(BF16)
    cum_wide, cum_thin = columns(mm(upto, decay_rows(dw[...], dn[...]), ((1,), (1,))))

    def normed(q, came, cum, inner, gain):
        kept = inner + mm(q[...], came[...]) * jnp.exp(cum)
        centered = kept - jnp.mean(kept, axis=-1, keepdims=True)
        power = jnp.mean(centered * centered, axis=-1, keepdims=True)
        return (centered * lax.rsqrt(power + EPS) * gain[...]).astype(BF16)

    wide = normed(qw, came_wide, cum_wide, within[:, :wide_width], gw)
    thin = normed(qn, came_thin, cum_thin, within[:, wide_width:], gn)
    outs = (far_a, far_b, right_a, right_b, left_a, left_b, own_a, own_b)
    rows, members = far_a.shape[0], length // (2 * far_a.shape[0])
    for m in range(members):
        spot = lax.rem(m - place[2] + members, members)
        order = jnp.where(spot == 2, 0, jnp.where(spot == 1, 1, jnp.where(spot == 3, 2, 3)))
        start = pl.multiple_of(order * 2 * rows, 2 * rows)
        turned_wide[pl.ds(start, 2 * rows), :] = wide[m * 2 * rows : (m + 1) * 2 * rows]
        turned_thin[pl.ds(start, 2 * rows), :] = thin[m * 2 * rows : (m + 1) * 2 * rows]
    step = 1024

    @pl.loop(0, ow.shape[1] // step)
    def _(n):
        cols = pl.ds(pl.multiple_of(n * step, step), step)
        done = (mm(turned_wide[...], ow[:, cols]) + mm(turned_thin[...], on[:, cols])).astype(BF16)
        for m, out in enumerate(outs):
            out[:, cols] = done[m * rows : (m + 1) * rows]


def add_two(a, b, c, d, first, second):
    first[...] = (a[...].astype(F32) + b[...].astype(F32)).astype(BF16)
    second[...] = (c[...].astype(F32) + d[...].astype(F32)).astype(BF16)


def rows_mid(
    own_a, left_a, right_a, own_b, left_b, right_b, stream, gain,
    mid_a, mid_b, normed_a, normed_b,
):
    rows = own_a.shape[0]
    halves = ((own_a, left_a, right_a, mid_a, normed_a), (own_b, left_b, right_b, mid_b, normed_b))
    for n, (own, left, right, middle, normed) in enumerate(halves):
        total = own[...].astype(F32) + left[...].astype(F32) + right[...].astype(F32)
        mid = (stream[n * rows : (n + 1) * rows].astype(F32) + total).astype(BF16)
        middle[...] = mid
        values = mid.astype(F32)
        power = jnp.mean(values * values, axis=-1, keepdims=True)
        normed[...] = (values * lax.rsqrt(power + EPS) * gain[...]).astype(BF16)


def fetched(pairs, sems):
    copies = [pltpu.make_async_copy(a, b, sems.at[n]) for n, (a, b) in enumerate(pairs)]
    for copy in copies:
        copy.start()
    return copies


def stacked(parts, rows):
    size = parts[0].shape[0]
    return [rows.at[pl.ds(n * size, size), :] for n in range(len(parts))]


def squared(x):
    raised = jnp.maximum(x, 0.0)
    return (raised * raised).astype(BF16)


def first_rows(*refs):
    *ends, up, down, rows, total, hidden, row_sems, up_sems, down_sems = refs
    number = len(ends) // 2
    parts, weights, outs = ends[:number], ends[number], ends[number + 1 :]
    size = parts[0].shape[0]
    units, block = up.shape[1], 512
    count = up.shape[0] // block

    def fetch(k, column, to, sems):
        span = pl.ds(pl.multiple_of(k * block, block), block)
        source = weights.at[span, pl.ds(column * units, units)]
        return pltpu.make_async_copy(source, to.at[span, :], sems.at[k])

    copies = fetched(list(zip(parts, stacked(parts, rows))), row_sems)

    @pl.loop(0, count)
    def _(k):
        fetch(k, 0, up, up_sems).start()

    @pl.loop(0, count)
    def _(k):
        fetch(k, 1, down, down_sems).start()

    for copy in copies:
        copy.wait()
    total[...] = jnp.zeros_like(total)

    @pl.loop(0, count)
    def _(k):
        fetch(k, 0, up, up_sems).wait()
        span = pl.ds(pl.multiple_of(k * block, block), block)
        total[...] += mm(rows[:, span], up[span, :])

    hidden[...] = squared(total[...])

    @pl.loop(0, count)
    def _(k):
        fetch(k, 1, down, down_sems).wait()
        span = pl.ds(pl.multiple_of(k * block, block), block)
        done = mm(hidden[...], down[span, :], ((1,), (1,))).astype(BF16)
        for m, out in enumerate(outs):
            out[:, span] = done[m * size : (m + 1) * size]


def more_rows(*refs):
    *ends, rows, hidden, row_sems = refs
    number = (len(ends) - 2) // 2
    parts, (up, down), outs = ends[:number], ends[number : number + 2], ends[number + 2 :]
    size, block = parts[0].shape[0], 1024
    for copy in fetched(list(zip(parts, stacked(parts, rows))), row_sems):
        copy.wait()

    @pl.loop(0, up.shape[1] // block)
    def _(n):
        cols = pl.ds(pl.multiple_of(n * block, block), block)
        hidden[:, cols] = squared(mm(rows[...], up[:, cols]))

    @pl.loop(0, down.shape[0] // block)
    def _(n):
        cols = pl.ds(pl.multiple_of(n * block, block), block)
        done = mm(hidden[...], down[cols, :], ((1,), (1,))).astype(BF16)
        for m, out in enumerate(outs):
            out[:, cols] = done[m * size : (m + 1) * size]


def first_forward(parts, weights):
    size, width = parts[0].shape
    units = weights.shape[1] // 2
    number = len(parts)
    count, total = width // 512, number * size
    far = pl.BlockSpec(memory_space=pltpu.HBM)
    held = [pltpu.with_memory_space_constraint(p, pltpu.HBM) for p in (*parts, weights)]
    *done, up, down = pl.pallas_call(
        first_rows,
        out_shape=[pltpu.VMEM((size, width), BF16)] * number
        + [pltpu.VMEM((width, units), BF16)] * 2,
        in_specs=[far] * (number + 1),
        out_specs=[vmem()] * (number + 2),
        scratch_shapes=[
            pltpu.VMEM((total, width), BF16),
            pltpu.VMEM((total, units), F32),
            pltpu.VMEM((total, units), BF16),
            pltpu.SemaphoreType.DMA((number,)),
            pltpu.SemaphoreType.DMA((count,)),
            pltpu.SemaphoreType.DMA((count,)),
        ],
        compiler_params=pltpu.CompilerParams(vmem_limit_bytes=20 * 2**20),
        cost_estimate=pl.CostEstimate(
            flops=4 * total * width * units, bytes_accessed=4 * units * width, transcendentals=0
        ),
        name="first_rows",
    )(*held)
    return done, (up, down)


def more_forward(parts, weights):
    size, width = parts[0].shape
    units = weights[0].shape[1]
    number = len(parts)
    total = number * size
    far = pl.BlockSpec(memory_space=pltpu.HBM)
    held = list(parts)
    held += [pltpu.with_memory_space_constraint(w, pltpu.VMEM) for w in weights]
    return pl.pallas_call(
        more_rows,
        out_shape=[shaped((size, width), BF16)] * number,
        in_specs=[pl.BlockSpec(memory_space=pl.ANY)] * number + [vmem()] * 2,
        out_specs=[vmem()] * number,
        scratch_shapes=[
            pltpu.VMEM((total, width), BF16),
            pltpu.VMEM((total, units), BF16),
            pltpu.SemaphoreType.DMA((number,)),
        ],
        compiler_params=pltpu.CompilerParams(vmem_limit_bytes=24 * 2**20),
        cost_estimate=pl.CostEstimate(
            flops=4 * total * width * units, bytes_accessed=4 * units * width, transcendentals=0
        ),
        name="more_rows",
    )(*held)


def with_middle(own_a, mid_a, own_b, mid_b, sum_a, sum_b):
    sum_a[...] = own_a[...].astype(F32) + mid_a[...].astype(F32)
    sum_b[...] = own_b[...].astype(F32) + mid_b[...].astype(F32)


def last_sum(sum_a, left_a, right_a, sum_b, left_b, right_b, out):
    rows = sum_a.shape[0]
    for n, parts in enumerate(((sum_a, left_a, right_a), (sum_b, left_b, right_b))):
        total = parts[0][...] + parts[1][...].astype(F32) + parts[2][...].astype(F32)
        out[n * rows : (n + 1) * rows] = total.astype(BF16)


def shift(x, axis, by, size, wrap=True):
    pairs = [(i, (i + by) % size) for i in range(size) if wrap or 0 <= i + by < size]
    return lax.ppermute(x, axis, pairs)


def swap(x):
    return lax.ppermute(x, "core", [(0, 1), (1, 0)])


def turn(x, by):
    return shift(x, "tp", by, lax.axis_size("tp"))


def sent_far(far_a, far_b):
    return turn(far_a, 1), turn(far_b, -1)


def sent_plain(right_b, left_a):
    return turn(right_b, 1), turn(left_a, -1)


def reduced(came_far, came_plain, right_a, left_b, near=False):
    like = [shaped(right_a.shape, BF16)] * 2
    held = (right_a, left_b) if near else (Far(right_a), Far(left_b))
    right_sum, left_sum = call(
        add_two, like, held[0], came_far[0], held[1], came_far[1], far_out=not near, limit=16
    )
    came = turn(right_sum, 1), *came_plain, turn(left_sum, -1)
    return came, right_sum


def spread(a, b):
    left_a, right_b = turn(a, 1), turn(b, -1)
    left_b, right_a = turn(b, 1), turn(a, -1)
    far_a, far_b = turn(left_a, 1), turn(right_b, -1)
    return far_a, far_b, right_a, right_b, left_a, left_b


def among(parts):
    return [parts[0]] + [shift(parts[d], "zb", d, 4) for d in range(1, 4)]


def on_device(
    stream_in, query_wide, key_wide, value_wide, query_narrow, key_narrow, value_narrow,
    decay_wide, decay_narrow, gain_wide, gain_narrow, out_wide, out_narrow, mlp_gain,
    up_weight, down_weight,
):
    members = lax.axis_size("tp")
    length, width = stream_in.shape
    portion = length // members
    member = lax.axis_index("tp")
    place = jnp.stack([lax.axis_index(n) for n in ("core", "zb", "tp")]).astype(jnp.int32)

    both = jnp.concatenate([up_weight, down_weight.T], axis=1)
    weights = lax.all_gather(both, SP, axis=0, tiled=True)

    wide_key, wide_value = key_wide.shape[1], value_wide.shape[1]
    thin_value = value_narrow.shape[1]
    half = wide_key // 2
    lanes = wide_value + 2 * LANES
    own = call(
        own_state, shaped((2, half, lanes), BF16),
        *map(Far, (key_wide, value_wide, decay_wide, key_narrow, value_narrow, decay_narrow)),
        flops=2 * length * wide_key * wide_value, moved=10**6,
    )
    sibling = swap(own)
    within = call(
        inside, shaped((length, wide_value + thin_value), F32),
        *map(Far, (query_wide, key_wide, value_wide, decay_wide)),
        *map(Far, (query_narrow, key_narrow, value_narrow, decay_narrow)),
        flops=6 * length * length * wide_value, moved=4 * 10**6,
    )
    rows = half // 4
    pieces = call(of_chip, shaped((4, rows, lanes), BF16), place, own, sibling)
    got = among([pieces[d] for d in range(4)])
    total = call(
        of_group, shaped((1, rows, lanes), BF16), place, *got,
        scratch=[pltpu.VMEM((4, rows, lanes), BF16)],
    )
    size = lax.axis_size("za")
    near, far = [shift(total, "za", d, size, wrap=False) for d in (1, 3)]
    mid = shift(near, "za", 1, size, wrap=False)
    found = call(
        before_each, shaped((4, rows, lanes - LANES), BF16), place, *got, near, mid, far,
        scratch=[pltpu.VMEM((4, rows, lanes), BF16), pltpu.VMEM((4, rows, lanes - LANES), BF16)],
    )
    back = among([found[d] for d in range(4)])
    own_half = call(gathered_half, shaped((half, lanes - LANES), BF16), place, *back)
    other_half = swap(own_half)
    quarter = portion // 2
    far_a, far_b, right_a, right_b, left_a, left_b, own_a, own_b = call(
        heads_out, [shaped((quarter, width), BF16)] * 8,
        place, own_half, other_half, sibling,
        *map(Far, (query_wide, query_narrow, decay_wide, decay_narrow)), within,
        *map(Far, (gain_wide[None], gain_narrow[None], out_wide, out_narrow)),
        scratch=[
            pltpu.VMEM((wide_key, wide_value), BF16),
            pltpu.VMEM((key_narrow.shape[1], thin_value), BF16),
            pltpu.VMEM((length, wide_value), BF16),
            pltpu.VMEM((length, thin_value), BF16),
        ],
        flops=4 * length * wide_value * width, moved=8 * 10**6, far_out=True,
    )
    came_far = sent_far(far_a, far_b)
    came, _ = reduced(came_far, sent_plain(right_b, left_a), right_a, left_b)
    from_left_a, from_left_b, from_right_a, from_right_b = came
    own_stream = lax.dynamic_slice_in_dim(stream_in, member * portion, portion, 0)
    mid_a, mid_b, normed_a, normed_b = call(
        rows_mid, [shaped((quarter, width), BF16)] * 4,
        Far(own_a), from_left_a, from_right_a, Far(own_b), from_left_b, from_right_b,
        Far(own_stream), Far(mlp_gain[None]), far_out=True, limit=16,
    )
    far_a, far_b, right_a, right_b, left_a, left_b = spread(normed_a, normed_b)
    done, kept = first_forward((far_a, far_b, right_b, left_a), weights)
    far_a, far_b, right_b, left_a = done
    came_far = sent_far(far_a, far_b)
    came_plain = sent_plain(right_b, left_a)
    right_a, left_b = more_forward((right_a, left_b), kept)
    came, sent = reduced(came_far, came_plain, right_a, left_b, near=True)
    from_left_a, from_left_b, from_right_a, from_right_b = came
    normed_a, normed_b, _ = lax.optimization_barrier((normed_a, normed_b, sent))
    own_a, own_b = more_forward((normed_a, normed_b), kept)
    sum_a, sum_b = call(
        with_middle, [shaped(mid_a.shape, F32)] * 2, own_a, Far(mid_a), own_b, Far(mid_b), limit=16
    )
    return call(
        last_sum, shaped((portion, width), BF16),
        sum_a, from_left_a, from_right_a, sum_b, from_left_b, from_right_b, far_out=True, limit=16,
    )


def solution(mesh):
    grp, sp, tp = mesh.shape["grp"], mesh.shape["sp"], mesh.shape["tp"]
    torus = Mesh(
        mesh.devices.reshape(grp, sp // 8, 4, 2, tp), ("grp", "za", "zb", "core", "tp")
    )
    placed = (
        P(GRP_SP, None),
        P(GRP_SP, "tp"),
        P(GRP_SP, "tp"),
        P(GRP_SP, "tp"),
        P(GRP_SP, "tp"),
        P(GRP_SP, "tp"),
        P(GRP_SP, "tp"),
        P("tp", GRP_SP),
        P("tp", GRP_SP),
        P("tp"),
        P("tp"),
        P("tp", None),
        P("tp", None),
        P(),
        P(SP, "tp"),
        P("tp", SP),
    )
    return jax.shard_map(
        on_device, mesh=torus, in_specs=placed, out_specs=P(GRP_SP_TP, None), check_vma=False
    )
```

```python
import jax
import jax.numpy as jnp
from jax import lax
from jax.experimental import pallas as pl
from jax.experimental.pallas import tpu as pltpu
from jax.sharding import Mesh
from jax.sharding import PartitionSpec as P

EPS = 1e-06
SP = ("za", "zb", "core")
GRP_SP = ("grp", "za", "zb", "core")
GRP_SP_TP = ("grp", "za", "zb", "core", "tp")
F32 = jnp.float32
BF16 = jnp.bfloat16
LANES = 128


def vmem():
    return pl.BlockSpec(memory_space=pltpu.VMEM)


def smem():
    return pl.BlockSpec(memory_space=pltpu.SMEM)


class Far:
    def __init__(self, x):
        self.x = x


def call(body, outs, *args, scratch=(), flops=0, moved=0, far_out=False, limit=48):
    many = isinstance(outs, (list, tuple))
    outs = list(outs) if many else [outs]
    pulled = [n for n, a in enumerate(args) if isinstance(a, Far)]
    args = [
        pltpu.with_memory_space_constraint(a.x, pltpu.HBM) if isinstance(a, Far) else a
        for a in args
    ]
    pushed = list(range(len(outs))) if far_out else []
    own = len(scratch)

    def inner(*refs):
        given, rest = list(refs[: len(args)]), list(refs[len(args) :])
        results, rest = rest[: len(outs)], rest[len(outs) :]
        kept, rest = rest[:own], rest[own:]
        held, sent = rest[: len(pulled)], rest[len(pulled) : len(pulled) + len(pushed)]
        sems = rest[-1]
        copies = []
        for k, n in enumerate(pulled):
            copies.append(pltpu.make_async_copy(given[n], held[k], sems.at[k]))
            copies[-1].start()
            given[n] = held[k]
        for copy in copies:
            copy.wait()
        body(*given, *(sent if pushed else results), *kept)
        copies = []
        for k in range(len(pushed)):
            copies.append(pltpu.make_async_copy(sent[k], results[k], sems.at[len(pulled) + k]))
            copies[-1].start()
        for copy in copies:
            copy.wait()

    far = pl.BlockSpec(memory_space=pltpu.HBM)
    specs = [
        smem() if a.dtype == jnp.int32 else far if n in pulled else vmem()
        for n, a in enumerate(args)
    ]
    buffers = [pltpu.VMEM(args[n].shape, args[n].dtype) for n in pulled]
    buffers += [pltpu.VMEM(outs[n].shape, outs[n].dtype) for n in pushed]
    result = pl.pallas_call(
        inner,
        out_shape=[pltpu.HBM(o.shape, o.dtype) for o in outs] if far_out else outs,
        in_specs=specs,
        out_specs=[far if far_out else vmem() for _ in outs],
        scratch_shapes=[
            *scratch, *buffers, pltpu.SemaphoreType.DMA((max(len(pulled) + len(pushed), 1),))
        ],
        compiler_params=pltpu.CompilerParams(vmem_limit_bytes=limit * 2**20),
        cost_estimate=pl.CostEstimate(flops=flops, bytes_accessed=moved, transcendentals=0),
        name=body.__name__,
    )(*args)
    return result if many else result[0]


def shaped(shape, dtype):
    return jax.ShapeDtypeStruct(shape, dtype)


def mm(a, b, dims=((1,), (0,))):
    return lax.dot_general(a, b, (dims, ((), ())), preferred_element_type=F32)


def three(x):
    high = x.astype(BF16).astype(F32)
    mid = (x - high).astype(BF16).astype(F32)
    low = (x - high - mid).astype(BF16).astype(F32)
    return high, mid, low


def pick(index, values):
    out = jnp.zeros_like(index, dtype=F32)
    for n, value in enumerate(values):
        out = jnp.where(index == n, value, out)
    return out


def decay_rows(dw, dn):
    row = lax.broadcasted_iota(jnp.int32, (8, dw.shape[1]), 0)
    return pick(row, three(dw) + three(dn)).astype(BF16)


def columns(table):
    wide = table[:, 0:1] + table[:, 1:2] + table[:, 2:3]
    thin = table[:, 3:4] + table[:, 4:5] + table[:, 5:6]
    return wide, thin


def log_lanes(wide, thin, rows):
    lane = lax.broadcasted_iota(jnp.int32, (rows, LANES), 1)
    return pick(lane, three(wide) + three(thin))


def positions(length):
    row = lax.broadcasted_iota(jnp.int32, (length, length), 0)
    col = lax.broadcasted_iota(jnp.int32, (length, length), 1)
    return row, col


def own_state(kw, vw, dw, kn, vn, dn, out):
    length = kw.shape[0]
    row, col = positions(length)
    later = (col > row).astype(F32).astype(BF16)
    table = decay_rows(dw[...], dn[...])
    end_wide, end_thin = columns(mm(later, table, ((1,), (1,))))
    total_wide = jnp.sum(dw[...], axis=1, keepdims=True)
    total_thin = jnp.sum(dn[...], axis=1, keepdims=True)

    def state(k, v, end):
        keyed = k[...].astype(F32) * k.shape[1] ** (-0.5) * jnp.exp(end)
        return mm(keyed.astype(BF16), v[...], ((0,), (0,))).astype(BF16)

    wide = state(kw, vw, end_wide)
    thin = state(kn, vn, end_thin)
    half_wide, half_thin = wide.shape[0] // 2, thin.shape[0] // 2
    at = wide.shape[1]
    logs = log_lanes(total_wide, total_thin, half_wide).astype(BF16)
    for h in range(2):
        out[h, :, :at] = wide[h * half_wide : (h + 1) * half_wide]
        part = thin[h * half_thin : (h + 1) * half_thin]
        out[h, :half_thin, at : at + LANES] = part[:, :LANES]
        out[h, half_thin:, at : at + LANES] = part[:, LANES:]
        out[h, :, at + LANES :] = logs


def inside(qw, kw, vw, dw, qn, kn, vn, dn, out):
    length = kw.shape[0]
    row, col = positions(length)
    causal = row >= col
    upto = causal.astype(F32).astype(BF16)
    table = decay_rows(dw[...], dn[...])
    col_wide, col_thin = columns(mm(upto, table, ((1,), (1,))))
    rows = mm(table, upto, ((1,), (1,)))
    row_wide = rows[0:1] + rows[1:2] + rows[2:3]
    row_thin = rows[3:4] + rows[4:5] + rows[5:6]

    def within(q, k, v, by_col, by_row):
        gap = jnp.where(causal, by_col - by_row, 0.0)
        fading = jnp.where(causal, jnp.exp(gap), 0.0)
        weights = mm(q[...], k[...], ((1,), (1,))) * k.shape[1] ** (-0.5) * fading
        return mm(weights.astype(BF16), v[...])

    at = vw.shape[1]
    out[:, :at] = within(qw, kw, vw, col_wide, row_wide)
    out[:, at:] = within(qn, kn, vn, col_thin, row_thin)


def unpack(x):
    x = x.astype(F32)
    cut = x.shape[-1] - LANES
    wide, thin = columns(x[:, cut:])
    return x[:, : cut - LANES], x[:, cut - LANES : cut], wide, thin


def after(earlier, latter):
    return (
        jnp.exp(latter[2]) * earlier[0] + latter[0],
        jnp.exp(latter[3]) * earlier[1] + latter[1],
        earlier[2] + latter[2],
        earlier[3] + latter[3],
    )


def put(ref, at, state, logs=True):
    rows, wide, thin = state[0].shape[0], state[0].shape[1], state[1].shape[1]
    ref[at, :, :wide] = state[0].astype(BF16)
    ref[at, :, wide : wide + thin] = state[1].astype(BF16)
    if logs:
        ref[at, :, wide + thin :] = log_lanes(state[2], state[3], rows).astype(BF16)


def of_chip(place, own, sibling, out):
    core, spot = place[0], place[1]
    first_core = core == 0
    pieces, rows = out.shape[0], out.shape[1]
    for d in range(pieces):
        start = pl.multiple_of(lax.rem(spot + d, pieces) * rows, rows)
        mine = own[core, pl.ds(start, rows), :]
        other = sibling[core, pl.ds(start, rows), :]
        first = jnp.where(first_core, mine, other)
        second = jnp.where(first_core, other, mine)
        put(out, d, after(unpack(first), unpack(second)))


def in_order(place, parts, ordered):
    pieces = len(parts)
    for d, part in enumerate(parts):
        ordered[lax.rem(place[1] - d + pieces, pieces)] = part[...]


def of_group(place, a, b, c, d, out, ordered):
    in_order(place, (a, b, c, d), ordered)
    total = unpack(ordered[0])
    for n in range(1, 4):
        total = after(total, unpack(ordered[n]))
    put(out, 0, total)


def before_each(place, a, b, c, d, near, mid, far, out, ordered, found):
    in_order(place, (a, b, c, d), ordered)
    state = after(after(unpack(far[0]), unpack(mid[0])), unpack(near[0]))
    for n in range(4):
        put(found, n, state, logs=False)
        state = after(state, unpack(ordered[n]))
    for n in range(4):
        out[n] = found[lax.rem(place[1] + n, 4)]


def gathered_half(place, a, b, c, d, out):
    parts = (a, b, c, d)
    rows = a.shape[0]
    for n, part in enumerate(parts):
        start = pl.multiple_of(lax.rem(place[1] - n + 4, 4) * rows, rows)
        out[pl.ds(start, rows), :] = part[...]


def heads_out(
    place, own_half, other_half, sibling, qw, qn, dw, dn, within, gw, gn, ow, on,
    far_a, far_b, right_a, right_b, left_a, left_b, own_a, own_b,
    came_wide, came_thin, turned_wide, turned_thin,
):
    first_core = place[0] == 0
    length = qw.shape[0]
    wide_width, thin_width = gw.shape[1], gn.shape[1]
    half_thin = came_thin.shape[0] // 2
    rows = own_half.shape[0]
    for h in range(2):
        mine = own_half[...] if h == 0 else other_half[...]
        other = other_half[...] if h == 0 else own_half[...]
        before = jnp.where(first_core, mine, other).astype(F32)
        s_wide, s_thin, l_wide, l_thin = unpack(sibling[h])
        b_wide, b_thin = before[:, :wide_width], before[:, wide_width:]
        wide = jnp.where(first_core, b_wide, jnp.exp(l_wide) * b_wide + s_wide)
        thin = jnp.where(first_core, b_thin, jnp.exp(l_thin) * b_thin + s_thin)
        came_wide[h * rows : (h + 1) * rows, :] = wide.astype(BF16)
        low = thin.astype(BF16)
        came_thin[h * half_thin : (h + 1) * half_thin, :LANES] = low[:half_thin]
        came_thin[h * half_thin : (h + 1) * half_thin, LANES:] = low[half_thin:]
    row, col = positions(length)
    upto = (row >= col).astype(F32).astype(BF16)
    cum_wide, cum_thin = columns(mm(upto, decay_rows(dw[...], dn[...]), ((1,), (1,))))

    def normed(q, came, cum, inner, gain):
        kept = inner + mm(q[...], came[...]) * jnp.exp(cum)
        centered = kept - jnp.mean(kept, axis=-1, keepdims=True)
        power = jnp.mean(centered * centered, axis=-1, keepdims=True)
        return (centered * lax.rsqrt(power + EPS) * gain[...]).astype(BF16)

    wide = normed(qw, came_wide, cum_wide, within[:, :wide_width], gw)
    thin = normed(qn, came_thin, cum_thin, within[:, wide_width:], gn)
    outs = (far_a, far_b, right_a, right_b, left_a, left_b, own_a, own_b)
    rows, members = far_a.shape[0], length // (2 * far_a.shape[0])
    for m in range(members):
        spot = lax.rem(m - place[2] + members, members)
        order = jnp.where(spot == 2, 0, jnp.where(spot == 1, 1, jnp.where(spot == 3, 2, 3)))
        start = pl.multiple_of(order * 2 * rows, 2 * rows)
        turned_wide[pl.ds(start, 2 * rows), :] = wide[m * 2 * rows : (m + 1) * 2 * rows]
        turned_thin[pl.ds(start, 2 * rows), :] = thin[m * 2 * rows : (m + 1) * 2 * rows]
    step = 512

    @pl.loop(0, ow.shape[1] // step)
    def _(n):
        cols = pl.ds(pl.multiple_of(n * step, step), step)
        done = (mm(turned_wide[...], ow[:, cols]) + mm(turned_thin[...], on[:, cols])).astype(BF16)
        for m, out in enumerate(outs):
            out[:, cols] = done[m * rows : (m + 1) * rows]


def add_two(a, b, c, d, first, second):
    first[...] = (a[...].astype(F32) + b[...].astype(F32)).astype(BF16)
    second[...] = (c[...].astype(F32) + d[...].astype(F32)).astype(BF16)


def rows_mid(
    own_a, left_a, right_a, own_b, left_b, right_b, stream, gain,
    mid_a, mid_b, normed_a, normed_b,
):
    rows = own_a.shape[0]
    halves = ((own_a, left_a, right_a, mid_a, normed_a), (own_b, left_b, right_b, mid_b, normed_b))
    for n, (own, left, right, middle, normed) in enumerate(halves):
        total = own[...].astype(F32) + left[...].astype(F32) + right[...].astype(F32)
        mid = (stream[n * rows : (n + 1) * rows].astype(F32) + total).astype(BF16)
        middle[...] = mid
        values = mid.astype(F32)
        power = jnp.mean(values * values, axis=-1, keepdims=True)
        normed[...] = (values * lax.rsqrt(power + EPS) * gain[...]).astype(BF16)


def fetched(pairs, sems):
    copies = [pltpu.make_async_copy(a, b, sems.at[n]) for n, (a, b) in enumerate(pairs)]
    for copy in copies:
        copy.start()
    return copies


def stacked(parts, rows):
    size = parts[0].shape[0]
    return [rows.at[pl.ds(n * size, size), :] for n in range(len(parts))]


def squared(x):
    raised = jnp.maximum(x, 0.0)
    return (raised * raised).astype(BF16)


def first_rows(*refs):
    *ends, up, down, rows, total, hidden, row_sems, up_sems, down_sems = refs
    number = len(ends) // 2
    parts, weights, outs = ends[:number], ends[number], ends[number + 1 :]
    size = parts[0].shape[0]
    units, block, wide = up.shape[1], 512, 1024

    def fetch(k, column, to, sems, block):
        span = pl.ds(pl.multiple_of(k * block, block), block)
        source = weights.at[span, pl.ds(column * units, units)]
        return pltpu.make_async_copy(source, to.at[span, :], sems.at[k])

    copies = fetched(list(zip(parts, stacked(parts, rows))), row_sems)

    @pl.loop(0, up.shape[0] // block)
    def _(k):
        fetch(k, 0, up, up_sems, block).start()

    @pl.loop(0, down.shape[0] // wide)
    def _(k):
        fetch(k, 1, down, down_sems, wide).start()

    for copy in copies:
        copy.wait()
    total[...] = jnp.zeros_like(total)

    @pl.loop(0, up.shape[0] // block)
    def _(k):
        fetch(k, 0, up, up_sems, block).wait()
        span = pl.ds(pl.multiple_of(k * block, block), block)
        total[...] += mm(rows[:, span], up[span, :])

    hidden[...] = squared(total[...])

    @pl.loop(0, down.shape[0] // wide)
    def _(k):
        fetch(k, 1, down, down_sems, wide).wait()
        span = pl.ds(pl.multiple_of(k * wide, wide), wide)
        done = mm(hidden[...], down[span, :], ((1,), (1,))).astype(BF16)
        for m, out in enumerate(outs):
            out[:, span] = done[m * size : (m + 1) * size]


def more_rows(*refs):
    *ends, rows, hidden = refs
    number = (len(ends) - 2) // 2
    parts, (up, down), outs = ends[:number], ends[number : number + 2], ends[number + 2 :]
    size, block = parts[0].shape[0], 1024
    for n, part in enumerate(parts):
        rows[n * size : (n + 1) * size, :] = part[...]

    @pl.loop(0, up.shape[1] // block)
    def _(n):
        cols = pl.ds(pl.multiple_of(n * block, block), block)
        hidden[:, cols] = squared(mm(rows[...], up[:, cols]))

    @pl.loop(0, down.shape[0] // block)
    def _(n):
        cols = pl.ds(pl.multiple_of(n * block, block), block)
        done = mm(hidden[...], down[cols, :], ((1,), (1,))).astype(BF16)
        for m, out in enumerate(outs):
            out[:, cols] = done[m * size : (m + 1) * size]


def first_forward(parts, weights):
    size, width = parts[0].shape
    units = weights.shape[1] // 2
    number = len(parts)
    total = number * size
    far = pl.BlockSpec(memory_space=pltpu.HBM)
    held = [pltpu.with_memory_space_constraint(p, pltpu.HBM) for p in (*parts, weights)]
    *done, up, down = pl.pallas_call(
        first_rows,
        out_shape=[pltpu.VMEM((size, width), BF16)] * number
        + [pltpu.VMEM((width, units), BF16)] * 2,
        in_specs=[far] * (number + 1),
        out_specs=[vmem()] * (number + 2),
        scratch_shapes=[
            pltpu.VMEM((total, width), BF16),
            pltpu.VMEM((total, units), F32),
            pltpu.VMEM((total, units), BF16),
            pltpu.SemaphoreType.DMA((number,)),
            pltpu.SemaphoreType.DMA((width // 512,)),
            pltpu.SemaphoreType.DMA((width // 1024,)),
        ],
        compiler_params=pltpu.CompilerParams(vmem_limit_bytes=20 * 2**20),
        cost_estimate=pl.CostEstimate(
            flops=4 * total * width * units, bytes_accessed=4 * units * width, transcendentals=0
        ),
        name="first_rows",
    )(*held)
    return done, (up, down)


def more_forward(parts, weights):
    size, width = parts[0].shape
    units = weights[0].shape[1]
    number = len(parts)
    total = number * size
    held = list(parts)
    held += [pltpu.with_memory_space_constraint(w, pltpu.VMEM) for w in weights]
    return pl.pallas_call(
        more_rows,
        out_shape=[shaped((size, width), BF16)] * number,
        in_specs=[vmem()] * (number + 2),
        out_specs=[vmem()] * number,
        scratch_shapes=[
            pltpu.VMEM((total, width), BF16),
            pltpu.VMEM((total, units), BF16),
        ],
        compiler_params=pltpu.CompilerParams(vmem_limit_bytes=24 * 2**20),
        cost_estimate=pl.CostEstimate(
            flops=4 * total * width * units, bytes_accessed=4 * units * width, transcendentals=0
        ),
        name="more_rows",
    )(*held)


def with_middle(own_a, mid_a, own_b, mid_b, sum_a, sum_b):
    sum_a[...] = own_a[...].astype(F32) + mid_a[...].astype(F32)
    sum_b[...] = own_b[...].astype(F32) + mid_b[...].astype(F32)


def last_sum(sum_a, left_a, right_a, sum_b, left_b, right_b, out):
    rows = sum_a.shape[0]
    for n, parts in enumerate(((sum_a, left_a, right_a), (sum_b, left_b, right_b))):
        total = parts[0][...] + parts[1][...].astype(F32) + parts[2][...].astype(F32)
        out[n * rows : (n + 1) * rows] = total.astype(BF16)


def shift(x, axis, by, size, wrap=True):
    pairs = [(i, (i + by) % size) for i in range(size) if wrap or 0 <= i + by < size]
    return lax.ppermute(x, axis, pairs)


def swap(x):
    return lax.ppermute(x, "core", [(0, 1), (1, 0)])


def turn(x, by):
    return shift(x, "tp", by, lax.axis_size("tp"))


def sent_far(far_a, far_b):
    return turn(far_a, 1), turn(far_b, -1)


def sent_plain(right_b, left_a):
    return turn(right_b, 1), turn(left_a, -1)


def reduced(came_far, came_plain, right_a, left_b, near=False):
    like = [shaped(right_a.shape, BF16)] * 2
    held = (right_a, left_b) if near else (Far(right_a), Far(left_b))
    right_sum, left_sum = call(
        add_two, like, held[0], came_far[0], held[1], came_far[1], far_out=not near, limit=16
    )
    came = turn(right_sum, 1), *came_plain, turn(left_sum, -1)
    return came, right_sum


def spread(a, b):
    left_a, right_b = turn(a, 1), turn(b, -1)
    left_b, right_a = turn(b, 1), turn(a, -1)
    far_a, far_b = turn(left_a, 1), turn(right_b, -1)
    return far_a, far_b, right_a, right_b, left_a, left_b


def among(parts):
    return [parts[0]] + [shift(parts[d], "zb", d, 4) for d in range(1, 4)]


def on_device(
    stream_in, query_wide, key_wide, value_wide, query_narrow, key_narrow, value_narrow,
    decay_wide, decay_narrow, gain_wide, gain_narrow, out_wide, out_narrow, mlp_gain,
    up_weight, down_weight,
):
    members = lax.axis_size("tp")
    length, width = stream_in.shape
    portion = length // members
    member = lax.axis_index("tp")
    place = jnp.stack([lax.axis_index(n) for n in ("core", "zb", "tp")]).astype(jnp.int32)

    both = jnp.concatenate([up_weight, down_weight.T], axis=1)
    weights = lax.all_gather(both, SP, axis=0, tiled=True)

    wide_key, wide_value = key_wide.shape[1], value_wide.shape[1]
    thin_value = value_narrow.shape[1]
    half = wide_key // 2
    lanes = wide_value + 2 * LANES
    own = call(
        own_state, shaped((2, half, lanes), BF16),
        *map(Far, (key_wide, value_wide, decay_wide, key_narrow, value_narrow, decay_narrow)),
        flops=2 * length * wide_key * wide_value, moved=10**6,
    )
    sibling = swap(own)
    within = call(
        inside, shaped((length, wide_value + thin_value), F32),
        *map(Far, (query_wide, key_wide, value_wide, decay_wide)),
        *map(Far, (query_narrow, key_narrow, value_narrow, decay_narrow)),
        flops=6 * length * length * wide_value, moved=4 * 10**6,
    )
    rows = half // 4
    pieces = call(of_chip, shaped((4, rows, lanes), BF16), place, own, sibling)
    got = among([pieces[d] for d in range(4)])
    total = call(
        of_group, shaped((1, rows, lanes), BF16), place, *got,
        scratch=[pltpu.VMEM((4, rows, lanes), BF16)],
    )
    size = lax.axis_size("za")
    near, far = [shift(total, "za", d, size, wrap=False) for d in (1, 3)]
    mid = shift(near, "za", 1, size, wrap=False)
    found = call(
        before_each, shaped((4, rows, lanes - LANES), BF16), place, *got, near, mid, far,
        scratch=[pltpu.VMEM((4, rows, lanes), BF16), pltpu.VMEM((4, rows, lanes - LANES), BF16)],
    )
    back = among([found[d] for d in range(4)])
    own_half = call(gathered_half, shaped((half, lanes - LANES), BF16), place, *back)
    other_half = swap(own_half)
    quarter = portion // 2
    far_a, far_b, right_a, right_b, left_a, left_b, own_a, own_b = call(
        heads_out, [shaped((quarter, width), BF16)] * 8,
        place, own_half, other_half, sibling,
        *map(Far, (query_wide, query_narrow, decay_wide, decay_narrow)), within,
        *map(Far, (gain_wide[None], gain_narrow[None], out_wide, out_narrow)),
        scratch=[
            pltpu.VMEM((wide_key, wide_value), BF16),
            pltpu.VMEM((key_narrow.shape[1], thin_value), BF16),
            pltpu.VMEM((length, wide_value), BF16),
            pltpu.VMEM((length, thin_value), BF16),
        ],
        flops=4 * length * wide_value * width, moved=8 * 10**6, far_out=True,
    )
    came_far = sent_far(far_a, far_b)
    came, _ = reduced(came_far, sent_plain(right_b, left_a), right_a, left_b)
    from_left_a, from_left_b, from_right_a, from_right_b = came
    own_stream = lax.dynamic_slice_in_dim(stream_in, member * portion, portion, 0)
    mid_a, mid_b, normed_a, normed_b = call(
        rows_mid, [shaped((quarter, width), BF16)] * 4,
        Far(own_a), from_left_a, from_right_a, Far(own_b), from_left_b, from_right_b,
        Far(own_stream), Far(mlp_gain[None]), far_out=True, limit=16,
    )
    far_a, far_b, right_a, right_b, left_a, left_b = spread(normed_a, normed_b)
    done, kept = first_forward((far_a, far_b, right_b, left_a), weights)
    far_a, far_b, right_b, left_a = done
    came_far = sent_far(far_a, far_b)
    came_plain = sent_plain(right_b, left_a)
    right_a, left_b = more_forward((right_a, left_b), kept)
    came, sent = reduced(came_far, came_plain, right_a, left_b, near=True)
    from_left_a, from_left_b, from_right_a, from_right_b = came
    normed_a, normed_b, _ = lax.optimization_barrier((normed_a, normed_b, sent))
    own_a, own_b = more_forward((normed_a, normed_b), kept)
    sum_a, sum_b = call(
        with_middle, [shaped(mid_a.shape, F32)] * 2, own_a, Far(mid_a), own_b, Far(mid_b), limit=16
    )
    return call(
        last_sum, shaped((portion, width), BF16),
        sum_a, from_left_a, from_right_a, sum_b, from_left_b, from_right_b, far_out=True, limit=16,
    )


def solution(mesh):
    grp, sp, tp = mesh.shape["grp"], mesh.shape["sp"], mesh.shape["tp"]
    torus = Mesh(
        mesh.devices.reshape(grp, sp // 8, 4, 2, tp), ("grp", "za", "zb", "core", "tp")
    )
    placed = (
        P(GRP_SP, None),
        P(GRP_SP, "tp"),
        P(GRP_SP, "tp"),
        P(GRP_SP, "tp"),
        P(GRP_SP, "tp"),
        P(GRP_SP, "tp"),
        P(GRP_SP, "tp"),
        P("tp", GRP_SP),
        P("tp", GRP_SP),
        P("tp"),
        P("tp"),
        P("tp", None),
        P("tp", None),
        P(),
        P(SP, "tp"),
        P("tp", SP),
    )
    return jax.shard_map(
        on_device, mesh=torus, in_specs=placed, out_specs=P(GRP_SP_TP, None), check_vma=False
    )
```
